256 devices in a mesh: fs: 32 (over z, y), tp: 8 (over x, core).
Axes of the slice: x: 4, y: 4, z: 8, core: 2. Of those that a mesh axis runs over, the one named last changes fastest.
Arguments:
- prompt: bfloat16 [24576, 2048], P('fs'), may hold values from -6 to 6
- routes: int32 [24576, 2], P('fs'), may hold values from 0 to 63, all different within a row; in each aligned block of 768 rows (0 to 767, 768 to 1535, ...) at most 48 rows name the same one
- affinity: float32 [24576, 2], P('fs'), may hold values from 0.05 to 1
- norm_gain: float32 [2048], P('fs'), may hold values from 0.1 to 1.9
- gate_master: float32 [64, 2048, 1024], P(None, 'fs', 'tp'), may hold values from -0.125 to 0.125
- up_master: float32 [64, 2048, 1024], P(None, 'fs', 'tp'), may hold values from -0.125 to 0.125
- down_master: float32 [64, 1024, 2048], P(None, 'fs', 'tp'), may hold values from -0.1875 to 0.1875
Outputs:
- mixed: bfloat16 [24576, 2048], P('fs', 'tp')
- gate_weights: bfloat16 [64, 2048, 1024], P('fs', None, 'tp')
- up_weights: bfloat16 [64, 2048, 1024], P('fs', None, 'tp')
- down_weights: bfloat16 [64, 1024, 2048], P('fs', None, 'tp')
The draws below stay inside these ranges and needn't reach their ends.
Inputs may be any that keep to these rules, and one draw needn't show every extreme that they name: `routes`: each row names 2 different experts. In each aligned block of 768 rows no expert is named more than 48 times, a bound that some block reaches.
All inputs are finite; a program needn't handle non-finite values.
Results may differ from the reference program's by a relative error of at most 0.0086.
Values may be sent and summed in bfloat16 or wider, within the bound.
A program may use at most 128 MiB of HBM per device.

```python
import math
import jax
import jax.numpy as jnp
import numpy as np
from jax import lax

D = 2048
FF = 1024
TOP = 2
TOK_DEV = 768
EXPERTS = 64
TOKENS = 24576
CAP = 48
N_FS = 32


def block_levels(key, extent, split, smallest, top_value):
    def one(position, parts):
        draws = jax.random.uniform(jax.random.fold_in(jax.random.fold_in(key, 6), position), (parts,), jnp.float32, smallest / len(split), top_value / len(split))
        return jnp.repeat(jnp.exp(draws), extent[position] // parts).reshape((-1,) + (1,) * (len(extent) - position - 1))

    level = one(*split[0])
    for cut in split[1:]:
        level = level * one(*cut)
    return level


def assign_block(key, own, number, rows, amount, top, most, slope):
    ranking = jax.random.permutation(key, amount)
    crowded, common = shares(amount, rows * top, most, slope, True), shares(amount, rows * top, most, slope, False)
    places = jnp.arange(amount)

    def named(lengths, turn):
        used = int((lengths > 0).sum())
        fixed = max(1, used // 4)
        moved = fixed + (places - fixed + turn * (used - fixed)) % max(1, amount - fixed)
        return jnp.zeros((amount,), jnp.int32).at[ranking[jnp.where(places < fixed, places, moved)]].set(jnp.asarray(lengths, jnp.int32))

    lengths = jnp.where(number % 4 == 0, named(crowded, number // 4), named(common, number - number // 4 - 1))
    mixed = jax.random.permutation(jax.random.fold_in(own, 3), amount)
    source_of, taker = mixed[0:amount // 2 * 2:2], mixed[1:amount // 2 * 2:2]
    margin = jnp.minimum(lengths[source_of] - 1, most - lengths[taker]) // 2
    margin = jnp.where((source_of == ranking[0]) | (taker == ranking[0]) | (lengths[taker] == 0), 0, jnp.maximum(margin, 0))
    moved = jax.random.randint(jax.random.fold_in(own, 4), (amount // 2,), 0, 1 << 20) % (margin + 1)
    lengths = lengths.at[source_of].add(-moved).at[taker].add(moved)
    labels = jnp.searchsorted(jnp.cumsum(lengths), jnp.arange(rows * top), side="right").astype(jnp.int32)
    grid = labels.reshape(top, rows).T
    grid = grid[jax.random.permutation(jax.random.fold_in(own, 1), rows)]
    turn = jax.random.randint(jax.random.fold_in(own, 2), (rows, 1), 0, top)
    return jnp.take_along_axis(grid, (jnp.arange(top)[None, :] + turn) % top, axis=1)


def shares(count, total, bound, slope, full):
    weights = [(1 << 20) // math.isqrt(rank ** slope) + 1 for rank in range(1, count + 1)]
    largest = bound if full else min(bound, max(-(-total // count), total * weights[0] // sum(weights)))
    least = 1 if total - largest >= count - 1 else 0
    counts, rest = [largest] + [least] * (count - 1), total - largest - least * (count - 1)
    while rest > 0:
        free = [i for i in range(1, count) if counts[i] < largest] or [i for i in range(1, count) if counts[i] < bound]
        whole, left = sum([weights[i] for i in free]), rest
        for i in free:
            extra = min(bound - counts[i], max(1, left * weights[i] // whole), rest)
            counts[i] = counts[i] + extra
            rest = rest - extra
    return np.array(counts)


def noise(rng, dims, width, most, pieces=(), kind=jnp.bfloat16):
    gain = block_levels(rng, dims, pieces, -0.22, 0.18) if pieces else 1.0
    drawn = jax.random.normal(rng, dims, jnp.float32) * width * gain
    return jnp.minimum(jnp.maximum(drawn, -most), most).astype(kind)


def setup_inputs(seed: int = 0) -> dict:
    arg_keys = jax.random.split(jax.random.key(seed), 8)
    prompt = noise(arg_keys[0], (TOKENS, D), 1.0, 6.0, ((0, 32),))
    routes_keys = jax.random.split(jax.random.fold_in(arg_keys[1], 1), TOKENS // TOK_DEV)
    routes_turns = jax.random.permutation(jax.random.fold_in(arg_keys[1], 3), TOKENS // TOK_DEV)
    routes = jax.vmap(lambda own, number: assign_block(jax.random.fold_in(arg_keys[1], 2), own, number, TOK_DEV, EXPERTS, TOP, CAP, 2))(routes_keys, routes_turns).reshape((TOKENS, TOP))
    affinity = jnp.clip(0.05 + 0.95 * jax.random.uniform(arg_keys[2], (TOKENS, TOP), jnp.float32) ** block_levels(arg_keys[2], (TOKENS, TOP), ((0, 32),), -0.2, 0.2), 0.05, 1.0)
    norm_gain = jnp.clip(1.0 + 0.18 * jax.random.normal(arg_keys[3], (D,), jnp.float32), 0.1, 1.9)
    gate_master = noise(arg_keys[4], (EXPERTS, D, FF), D ** -0.5, 0.125, ((1, 32), (2, 8)), jnp.float32)
    up_master = noise(arg_keys[5], (EXPERTS, D, FF), D ** -0.5, 0.125, ((1, 32), (2, 8)), jnp.float32)
    down_master = noise(arg_keys[6], (EXPERTS, FF, D), FF ** -0.5, 0.1875, ((1, 32), (2, 8)), jnp.float32)
    return {"prompt": prompt, "routes": routes, "affinity": affinity, "norm_gain": norm_gain, "gate_master": gate_master, "up_master": up_master, "down_master": down_master}


norm_eps = 1e-06

def one_expert(operands):
    slot_rows, gate_weight, up_weight, down_weight = operands
    gate_pre = jnp.dot(slot_rows, gate_weight, preferred_element_type=jnp.float32)
    up_pre = jnp.dot(slot_rows, up_weight, preferred_element_type=jnp.float32)
    hidden = (jax.nn.silu(gate_pre) * up_pre).astype(jnp.bfloat16)
    return jnp.dot(hidden, down_weight, preferred_element_type=jnp.float32).astype(jnp.bfloat16)

def reference(prompt, routes, affinity, norm_gain, gate_master, up_master, down_master):
    gain_rows = norm_gain[None, :, None]
    gate_weights = (gate_master * gain_rows).astype(jnp.bfloat16)
    up_weights = (up_master * gain_rows).astype(jnp.bfloat16)
    down_weights = down_master.astype(jnp.bfloat16)
    values = prompt.astype(jnp.float32)
    normed = (values * lax.rsqrt(lax.optimization_barrier(jnp.mean(values * values, axis=-1, keepdims=True)) + norm_eps)).astype(jnp.bfloat16)
    flat_ids = routes.reshape(N_FS, TOK_DEV * TOP)
    onehot = (flat_ids[:, :, None] == jnp.arange(EXPERTS, dtype=jnp.int32)[None, None, :]).astype(jnp.int32)
    slot_rank = lax.optimization_barrier(jnp.sum(jnp.cumsum(onehot, axis=1) * onehot, axis=2)) - 1
    column = (jnp.arange(N_FS, dtype=jnp.int32)[:, None] * CAP + slot_rank).reshape(-1).astype(jnp.int32)
    expert_of = flat_ids.reshape(-1).astype(jnp.int32)
    token_of = (jnp.arange(TOKENS * TOP, dtype=jnp.int32) // TOP).astype(jnp.int32)
    buffer = jnp.zeros((EXPERTS, N_FS * CAP, D), jnp.bfloat16).at[expert_of, column].set(normed[token_of])
    outputs = lax.map(one_expert, (buffer, gate_weights, up_weights, down_weights))
    picked = outputs[expert_of, column].reshape(TOKENS, TOP, D).astype(jnp.float32)
    share = affinity / lax.optimization_barrier(jnp.sum(affinity, axis=1, keepdims=True))
    mixed = lax.optimization_barrier(jnp.sum(share[:, :, None] * picked, axis=1)).astype(jnp.bfloat16)
    return (mixed, gate_weights, up_weights, down_weights)
```

```python
import jax
import jax.numpy as jnp
from jax import lax
from jax.experimental import pallas as pl
from jax.experimental.pallas import tpu as pltpu
from jax.sharding import PartitionSpec as P

MESH = pl.DeviceIdType.MESH
norm_eps = 1e-06

NZ, NY, NX = 8, 4, 4
NFS = NZ * NY
NTP = NX * 2
CAP = 48
BF16, F32 = jnp.bfloat16, jnp.float32


def plane_step(i):
    return 4 + ((i + 1) // 2) * (1 - 2 * (i % 2))


def loop(count, body):
    def step(i, carry):
        body(i)
        return carry

    lax.fori_loop(0, count, step, 0)


def kernel(
    rt_ref, at_ref, gain_ref, prompt_ref, gate_ref, up_ref, down_ref,
    mixed_ref, gate_out, up_out, down_out,
    pbuf, gbuf, ubuf, dbuf, wsend_gu, wsend_d, nm, outbox, tok, wgu, wd, hid, eo, ret, wcomb, macc,
    slots, load_sem, out_sem, swgu, swd, rwgu, rwd, st, sx, own, xl, xr, fl, fr, po, pl_, pr, pf,
    sh, hxl, hxr, hfl, hfr, hpo, hpl, hpr, hpf, sr, rr,
):
    me = lax.axis_index("fs")
    t = lax.axis_index("tp")
    mz, my = me // NY, me % NY
    mx, mc = t // 2, t % 2
    right = ((mx + 1) % NX) * 2 + mc
    left = ((mx + NX - 1) % NX) * 2 + mc
    far = ((mx + 2) % NX) * 2 + mc
    mate = mx * 2 + 1 - mc

    def load(n, src, dst):
        return pltpu.make_async_copy(src, dst, load_sem.at[n])

    loads = [
        load(0, gate_ref.at[:, 0], gbuf.at[0]),
        load(1, up_ref.at[:, 0], ubuf.at[0]),
        load(2, prompt_ref, pbuf),
        load(3, down_ref.at[:, 0], dbuf.at[0]),
        load(4, gate_ref.at[:, 1], gbuf.at[1]),
        load(5, up_ref.at[:, 1], ubuf.at[1]),
        load(6, down_ref.at[:, 1], dbuf.at[1]),
    ]
    for l in loads:
        l.start()

    barrier = pltpu.get_barrier_semaphore()

    def greet(i):
        pl.semaphore_signal(barrier, inc=1, device_id=((me + 1 + i) % NFS, t), device_id_type=MESH)

    loop(NFS - 1, greet)
    for other in (right, left, mate):
        pl.semaphore_signal(barrier, inc=1, device_id=(me, other), device_id_type=MESH)

    def remote(src, dst, ssem, rsem, fs, tp):
        return pltpu.make_async_remote_copy(
            src_ref=src, dst_ref=dst, send_sem=ssem, recv_sem=rsem, device_id=(fs, tp), device_id_type=MESH
        )

    def got(ref, sem):
        remote(ref, ref, sem, sem, me, t).wait_recv()

    def sent(ref, sem):
        remote(ref, ref, sem, sem, me, t).wait_send()

    def to_peers(send):
        def plane(i):
            z = (mz + plane_step(i)) % NZ
            for dy in range(NY):
                dst = z * NY + (my + dy) % NY
                if dy == 0:
                    @pl.when(i < NZ - 1)
                    def _():
                        send(dst)
                else:
                    send(dst)

        loop(NZ, plane)

    def cast_gu(e):
        loads[0 if e == 0 else 4].wait()
        loads[1 if e == 0 else 5].wait()

        def block(b):
            rows = pl.ds(b * 4, 4)
            gain = gain_ref[...][None]
            wsend_gu[e, rows, :, 0:128] = (gbuf[e, rows] * gain).astype(BF16)
            wsend_gu[e, rows, :, 128:256] = (ubuf[e, rows] * gain).astype(BF16)

        loop(8, block)
        wgu[e, pl.ds(pl.multiple_of(me * 64, 64), 64), :] = wsend_gu[e, me]

    def send_gu(e):
        def send(dst):
            remote(
                wsend_gu.at[e, dst], wgu.at[e, pl.ds(pl.multiple_of(me * 64, 64), 64)], swgu.at[e], rwgu.at[e], dst, t
            ).start()

        to_peers(send)

    def cast_d(e):
        loads[3 if e == 0 else 6].wait()

        def block(b):
            rows = pl.ds(b * 4, 4)
            wsend_d[e, rows] = dbuf[e, rows].astype(BF16)

        loop(8, block)
        wd[e, pl.ds(pl.multiple_of(me * 32, 32), 32), :] = wsend_d[e, me]

    def send_d(e):
        def send(dst):
            remote(
                wsend_d.at[e, dst], wd.at[e, pl.ds(pl.multiple_of(me * 32, 32), 32)], swd.at[e], rwd.at[e], dst, t
            ).start()

        to_peers(send)

    cast_gu(0)
    pl.semaphore_wait(barrier, NFS - 1 + 3)
    send_gu(0)

    r0, r1 = rt_ref[0:1, :], rt_ref[1:2, :]
    experts = lax.broadcasted_iota(jnp.int32, (64, 768), 0)
    oh0 = (experts == r0).astype(F32)
    oh1 = (experts == r1).astype(F32)
    before = lax.broadcasted_iota(jnp.int32, (768, 768), 0) < lax.broadcasted_iota(jnp.int32, (768, 768), 1)
    count = jnp.dot((oh0 + oh1).astype(BF16), before.astype(F32).astype(BF16), preferred_element_type=F32)
    rank0 = jnp.sum(count * oh0, axis=0, keepdims=True).astype(jnp.int32)
    rank1 = jnp.sum(count * oh1, axis=0, keepdims=True).astype(jnp.int32)
    slots[0:1, :] = r0 * CAP + rank0
    slots[1:2, :] = r1 * CAP + rank1

    loads[2].wait()

    def norm(b):
        rows = pl.ds(pl.multiple_of(b * 64, 64), 64)
        x = pbuf[rows, :].astype(F32)
        scale = lax.rsqrt(jnp.mean(x * x, axis=-1, keepdims=True) + norm_eps)
        mine = pbuf[rows, pl.ds(pl.multiple_of(t * 256, 256), 256)].astype(F32)
        nm[rows, :] = (mine * scale).astype(BF16)

    loop(12, norm)

    def build(i):
        z = (mz + plane_step(i)) % NZ
        index = lax.broadcasted_iota(jnp.int32, (8 * CAP, 768), 0) + z * (8 * CAP)
        hit = (index == slots[0:1, :]) | (index == slots[1:2, :])
        rows = jnp.dot(hit.astype(F32).astype(BF16), nm[...], preferred_element_type=F32)
        outbox[pl.ds(z * 8, 8)] = rows.astype(BF16).reshape(8, CAP, 256)

    def send_t(i):
        z = (mz + plane_step(i)) % NZ
        for dy in range(NY):
            dst = z * NY + (my + dy) % NY

            def go(dst=dst):
                remote(outbox.at[pl.ds(dst * 2, 2)], tok.at[t, me], st, own.at[i], dst, t).start()

            if dy == 0:
                pl.when(i < NZ - 1)(go)
            else:
                go()

    def dispatch(i):
        build(i)

        @pl.when(i > 0)
        def _():
            send_t(i - 1)

    loop(NZ, dispatch)
    tok[t, me] = outbox[pl.ds(me * 2, 2)]
    cast_d(0)
    send_t(NZ - 1)
    send_d(0)
    cast_gu(1)
    cast_d(1)
    send_gu(1)
    send_d(1)

    a0, a1 = at_ref[0:1, :], at_ref[1:2, :]
    total = a0 + a1

    def keys(r, rank, e):
        key = jnp.right_shift(r, 1) * CAP + rank
        return jnp.where(jnp.bitwise_and(r, 1) == e, key, -1).astype(F32)

    packed = jnp.concatenate(
        [keys(r0, rank0, 0), keys(r1, rank1, 0), keys(r0, rank0, 1), keys(r1, rank1, 1), a0 / total, a1 / total,
         jnp.zeros((122, 768), F32)],
        axis=0,
    )
    macc[...] = jnp.concatenate([packed.T, jnp.zeros((768, 128), F32)], axis=1)

    def weigh(b):
        rows = pl.ds(pl.multiple_of(b * 64, 64), 64)
        columns = macc[rows, 0:128]
        index = lax.broadcasted_iota(jnp.int32, (64, NFS * CAP), 1).astype(F32)
        for e in range(2):
            first = jnp.where(index == columns[:, 2 * e : 2 * e + 1], columns[:, 4:5], 0.0)
            second = jnp.where(index == columns[:, 2 * e + 1 : 2 * e + 2], columns[:, 5:6], 0.0)
            wcomb[e, rows, :] = (first + second).astype(BF16)

    loop(12, weigh)

    def plane_rows(i):
        z = (mz + NZ - plane_step(i)) % NZ
        return z * NY

    def gather(i):
        @pl.when(i < NZ)
        def _():
            at = plane_rows(i)

            @pl.when(i < NZ - 1)
            def _():
                got(tok.at[t, pl.ds(at, NY)], own.at[i])

            @pl.when(i == NZ - 1)
            def _():
                got(tok.at[t, pl.ds(at, NY - 1)], own.at[i])

            piece = tok.at[t, pl.ds(at, NY)]
            remote(piece, piece, sx, xl.at[i], me, right).start()
            remote(piece, piece, sx, xr.at[i], me, left).start()
            remote(piece, piece, sx, po.at[i], me, mate).start()

        @pl.when((i >= 1) & (i < NZ + 1))
        def _():
            j = i - 1
            at = plane_rows(j)
            whole = tok.at[left, pl.ds(at, NY)]
            half = tok.at[left, pl.ds(at, NY // 2)]
            got(whole, xl.at[j])
            remote(half, half, sx, fl.at[j], me, right).start()
            remote(whole, whole, sx, pl_.at[j], me, mate).start()
            whole = tok.at[right, pl.ds(at, NY)]
            half = tok.at[right, pl.ds(at + NY // 2, NY // 2)]
            got(whole, xr.at[j])
            remote(half, half, sx, fr.at[j], me, left).start()
            remote(whole, whole, sx, pr.at[j], me, mate).start()

        @pl.when(i >= 2)
        def _():
            j = i - 2
            at = plane_rows(j)
            whole = tok.at[far, pl.ds(at, NY)]
            got(tok.at[far, pl.ds(at, NY // 2)], fl.at[j])
            got(tok.at[far, pl.ds(at + NY // 2, NY // 2)], fr.at[j])
            remote(whole, whole, sx, pf.at[j], me, mate).start()

    loop(NZ + 2, gather)

    def gathered(i):
        at = pl.ds(plane_rows(i), NY)
        got(tok.at[mate, at], po.at[i])
        got(tok.at[left + 1 - 2 * mc, at], pl_.at[i])
        got(tok.at[right + 1 - 2 * mc, at], pr.at[i])
        got(tok.at[far + 1 - 2 * mc, at], pf.at[i])

    loop(NZ, gathered)

    CH = 8
    NCH = NFS // CH
    CR = CH * CAP

    def chunk_of(k):
        step = (2 + ((k + 1) // 2) * (1 - 2 * (k % 2))) % NCH
        return (mz // 2 + step) % NCH

    def expert(e):
        got(wsend_gu.at[e, pl.ds(0, NFS - 1)], rwgu.at[e])
        pltpu.make_async_copy(wgu.at[e, :, pl.ds(0, 128)], gate_out.at[e], out_sem.at[3 * e]).start()
        pltpu.make_async_copy(wgu.at[e, :, pl.ds(128, 128)], up_out.at[e], out_sem.at[3 * e + 1]).start()

        def hrows(k):
            return pl.ds(pl.multiple_of(chunk_of(k) * CR, CR), CR)

        def send_h(k):
            piece = hid.at[t, e, hrows(k)]
            remote(piece, piece, sh.at[e], hxl.at[e, k], me, right).start()
            remote(piece, piece, sh.at[e], hxr.at[e, k], me, left).start()
            remote(piece, piece, sh.at[e], hpo.at[e, k], me, mate).start()

        def forward_h(k):
            base = pl.multiple_of(chunk_of(k) * CR, CR)
            whole = hid.at[left, e, pl.ds(base, CR)]
            half = hid.at[left, e, pl.ds(base, CR // 2)]
            got(whole, hxl.at[e, k])
            remote(half, half, sh.at[e], hfl.at[e, k], me, right).start()
            remote(whole, whole, sh.at[e], hpl.at[e, k], me, mate).start()
            whole = hid.at[right, e, pl.ds(base, CR)]
            half = hid.at[right, e, pl.ds(base + CR // 2, CR // 2)]
            got(whole, hxr.at[e, k])
            remote(half, half, sh.at[e], hfr.at[e, k], me, left).start()
            remote(whole, whole, sh.at[e], hpr.at[e, k], me, mate).start()

        def pass_h(k):
            base = pl.multiple_of(chunk_of(k) * CR, CR)
            whole = hid.at[far, e, pl.ds(base, CR)]
            got(hid.at[far, e, pl.ds(base, CR // 2)], hfl.at[e, k])
            got(hid.at[far, e, pl.ds(base + CR // 2, CR // 2)], hfr.at[e, k])
            remote(whole, whole, sh.at[e], hpf.at[e, k], me, mate).start()

        def up_step(k):
            @pl.when(k < NCH)
            def _():
                senders = pl.ds(chunk_of(k) * CH, CH)
                acc = jnp.zeros((CR, 256), F32)
                for p in range(NTP):
                    x = tok[p, senders, e].reshape(CR, 256)
                    acc = acc + jnp.dot(x, wgu[e, p * 256 : (p + 1) * 256, :], preferred_element_type=F32)
                gate, up = acc[:, 0:128], acc[:, 128:256]
                hid[t, e, hrows(k), :] = (gate / (1.0 + jnp.exp(-gate)) * up).astype(BF16)

            @pl.when((k >= 1) & (k < NCH + 1))
            def _():
                send_h(k - 1)

            @pl.when((k >= 2) & (k < NCH + 2))
            def _():
                forward_h(k - 2)

            @pl.when(k >= 3)
            def _():
                pass_h(k - 3)

        loop(NCH + 3, up_step)

        got(wsend_d.at[e, pl.ds(0, NFS - 1)], rwd.at[e])
        pltpu.make_async_copy(wd.at[e], down_out.at[e], out_sem.at[3 * e + 2]).start()

        def send_r(k):
            plane = chunk_of(k) * 2
            for n in range(CH):
                s = (plane + n // NY) * NY + (my + n) % NY

                def go(s=s):
                    remote(eo.at[e, s], ret.at[e, me], sr.at[e], rr.at[e], s, t).start()

                if n % NY == 0:
                    pl.when(s != me)(go)
                else:
                    go()

        def down_step(k):
            @pl.when(k < NCH)
            def _():
                rows = hrows(k)
                got(hid.at[mate, e, rows], hpo.at[e, k])
                got(hid.at[left + 1 - 2 * mc, e, rows], hpl.at[e, k])
                got(hid.at[right + 1 - 2 * mc, e, rows], hpr.at[e, k])
                got(hid.at[far + 1 - 2 * mc, e, rows], hpf.at[e, k])
                acc = jnp.zeros((CR, 256), F32)
                for q in range(NX):
                    h = jnp.concatenate([hid[2 * q, e, rows, :], hid[2 * q + 1, e, rows, :]], axis=1)
                    acc = acc + jnp.dot(h, wd[e, q * 256 : (q + 1) * 256, :], preferred_element_type=F32)
                eo[e, pl.ds(chunk_of(k) * CH, CH)] = acc.astype(BF16).reshape(CH, CAP, 256)

            @pl.when(k >= 1)
            def _():
                send_r(k - 1)

        loop(NCH + 1, down_step)
        ret[e, me] = eo[e, me]

    expert(0)
    expert(1)

    got(ret.at[0, pl.ds(0, NFS - 1)], rr.at[0])

    def mix_first(b):
        rows = pl.ds(pl.multiple_of(b * 256, 256), 256)
        macc[rows, :] = jnp.dot(wcomb[0, rows, :], ret[0].reshape(NFS * CAP, 256), preferred_element_type=F32)

    loop(3, mix_first)
    got(ret.at[1, pl.ds(0, NFS - 1)], rr.at[1])

    def mix_second(b):
        rows = pl.ds(pl.multiple_of(b * 256, 256), 256)
        both = macc[rows, :] + jnp.dot(wcomb[1, rows, :], ret[1].reshape(NFS * CAP, 256), preferred_element_type=F32)
        mixed_ref[rows, :] = both.astype(BF16)

    loop(3, mix_second)

    for e in range(2):
        sent(wsend_gu.at[e, pl.ds(0, NFS - 1)], swgu.at[e])
        sent(wsend_d.at[e, pl.ds(0, NFS - 1)], swd.at[e])
        sent(hid.at[pl.ds(0, 7), e], sh.at[e])
        sent(eo.at[e, pl.ds(0, NFS - 1)], sr.at[e])
        pltpu.make_async_copy(wgu.at[e, :, pl.ds(0, 128)], gate_out.at[e], out_sem.at[3 * e]).wait()
        pltpu.make_async_copy(wgu.at[e, :, pl.ds(128, 128)], up_out.at[e], out_sem.at[3 * e + 1]).wait()
        pltpu.make_async_copy(wd.at[e], down_out.at[e], out_sem.at[3 * e + 2]).wait()
    sent(outbox.at[pl.ds(0, 2 * (NFS - 1))], st)
    sent(tok.at[pl.ds(0, 7)], sx)


def per_device(prompt, routes, affinity, norm_gain, gate_master, up_master, down_master):
    vmem = pl.BlockSpec(memory_space=pltpu.VMEM)
    hbm = pl.BlockSpec(memory_space=pl.ANY)
    dma = pltpu.SemaphoreType.DMA
    scratch = [
        pltpu.VMEM((768, 2048), BF16),
        pltpu.VMEM((2, 32, 64, 128), F32),
        pltpu.VMEM((2, 32, 64, 128), F32),
        pltpu.VMEM((2, 32, 32, 256), F32),
        pltpu.VMEM((2, 32, 64, 256), BF16),
        pltpu.VMEM((2, 32, 32, 256), BF16),
        pltpu.VMEM((768, 256), BF16),
        pltpu.VMEM((64, CAP, 256), BF16),
        pltpu.VMEM((NTP, NFS, 2, CAP, 256), BF16),
        pltpu.VMEM((2, 2048, 256), BF16),
        pltpu.VMEM((2, 1024, 256), BF16),
        pltpu.VMEM((NTP, 2, NFS * CAP, 128), BF16),
        pltpu.VMEM((2, NFS, CAP, 256), BF16),
        pltpu.VMEM((2, NFS, CAP, 256), BF16),
        pltpu.VMEM((2, 768, NFS * CAP), BF16),
        pltpu.VMEM((768, 256), F32),
        pltpu.VMEM((8, 768), jnp.int32),
        dma((7,)),
        dma((6,)),
        dma((2,)), dma((2,)), dma((2,)), dma((2,)),
        dma, dma,
        *[dma((NZ,)) for _ in range(9)],
        dma((2,)),
        *[dma((2, 4)) for _ in range(8)],
        dma((2,)), dma((2,)),
    ]
    return pl.pallas_call(
        kernel,
        out_shape=(
            jax.ShapeDtypeStruct((768, 256), BF16),
            jax.ShapeDtypeStruct((2, 2048, 128), BF16),
            jax.ShapeDtypeStruct((2, 2048, 128), BF16),
            jax.ShapeDtypeStruct((2, 1024, 256), BF16),
        ),
        in_specs=[vmem] * 3 + [hbm] * 4,
        out_specs=(vmem, hbm, hbm, hbm),
        scratch_shapes=scratch,
        compiler_params=pltpu.CompilerParams(
            collective_id=0, has_side_effects=True, vmem_limit_bytes=60 * 1024 * 1024
        ),
        name="hand_off",
    )(
        routes.T,
        affinity.T,
        jnp.broadcast_to(norm_gain[:, None], (64, 128)),
        prompt,
        gate_master.reshape(32, 2, 64, 128),
        up_master.reshape(32, 2, 64, 128),
        down_master.reshape(32, 2, 32, 256),
    )


def solution(mesh):
    in_specs = (
        P("fs", None),
        P("fs", None),
        P("fs", None),
        P("fs"),
        P(None, "fs", "tp"),
        P(None, "fs", "tp"),
        P(None, "fs", "tp"),
    )
    out_specs = (P("fs", "tp"), P("fs", None, "tp"), P("fs", None, "tp"), P("fs", None, "tp"))
    return jax.shard_map(
        per_device, mesh=mesh, in_specs=in_specs, out_specs=out_specs, check_vma=False
    )
```

```python
import jax
import jax.numpy as jnp
from jax import lax
from jax.experimental import pallas as pl
from jax.experimental.pallas import tpu as pltpu
from jax.sharding import PartitionSpec as P

MESH = pl.DeviceIdType.MESH
norm_eps = 1e-06

NZ, NY, NX = 8, 4, 4
NFS = NZ * NY
NTP = NX * 2
CAP = 48
BF16, F32 = jnp.bfloat16, jnp.float32


def plane_step(i):
    return NZ + ((i + 1) // 2) * (2 * (i % 2) - 1)


def loop(count, body):
    def step(i, carry):
        body(i)
        return carry

    lax.fori_loop(0, count, step, 0)


def kernel(
    rt_ref, at_ref, gain_ref, prompt_ref, gate_ref, up_ref, down_ref,
    mixed_ref, gate_out, up_out, down_out,
    pbuf, gbuf, ubuf, dbuf, wsend_gu, wsend_d, nm, outbox, tok, wgu, wd, hid, eo, ret, wcomb, macc,
    slots, load_sem, out_sem, swgu, swd, rwgu, rwd, st, sx, own, xl, xr, fl, fr, po, pl_, pr, pf,
    sh, hxl, hxr, hfl, hfr, hpo, hpl, hpr, hpf, sr, rr,
):
    me = lax.axis_index("fs")
    t = lax.axis_index("tp")
    mz, my = me // NY, me % NY
    mx, mc = t // 2, t % 2
    right = ((mx + 1) % NX) * 2 + mc
    left = ((mx + NX - 1) % NX) * 2 + mc
    far = ((mx + 2) % NX) * 2 + mc
    mate = mx * 2 + 1 - mc

    def load(n, src, dst):
        return pltpu.make_async_copy(src, dst, load_sem.at[n])

    loads = [
        load(3, down_ref.at[:, 0], dbuf.at[0]),
        load(2, prompt_ref, pbuf),
        load(0, gate_ref.at[:, 0], gbuf.at[0]),
        load(1, up_ref.at[:, 0], ubuf.at[0]),
        load(4, gate_ref.at[:, 1], gbuf.at[1]),
        load(5, up_ref.at[:, 1], ubuf.at[1]),
        load(6, down_ref.at[:, 1], dbuf.at[1]),
    ]
    for l in loads:
        l.start()

    barrier = pltpu.get_barrier_semaphore()

    def greet(i):
        pl.semaphore_signal(barrier, inc=1, device_id=((me + 1 + i) % NFS, t), device_id_type=MESH)

    loop(NFS - 1, greet)
    for other in (right, left, mate):
        pl.semaphore_signal(barrier, inc=1, device_id=(me, other), device_id_type=MESH)

    def remote(src, dst, ssem, rsem, fs, tp):
        return pltpu.make_async_remote_copy(
            src_ref=src, dst_ref=dst, send_sem=ssem, recv_sem=rsem, device_id=(fs, tp), device_id_type=MESH
        )

    def got(ref, sem):
        remote(ref, ref, sem, sem, me, t).wait_recv()

    def sent(ref, sem):
        remote(ref, ref, sem, sem, me, t).wait_send()

    def to_peers(send):
        def plane(i):
            z = (mz + plane_step(i)) % NZ
            for dy in range(NY):
                dst = z * NY + (my + dy) % NY
                if dy == 0:
                    @pl.when(i > 0)
                    def _():
                        send(dst)
                else:
                    send(dst)

        loop(NZ, plane)

    def cast_gu(e):
        loads[2 if e == 0 else 4].wait()
        loads[3 if e == 0 else 5].wait()

        def block(b):
            rows = pl.ds(b * 4, 4)
            gain = gain_ref[...][None]
            wsend_gu[e, rows, :, 0:128] = (gbuf[e, rows] * gain).astype(BF16)
            wsend_gu[e, rows, :, 128:256] = (ubuf[e, rows] * gain).astype(BF16)

        loop(8, block)
        wgu[e, pl.ds(pl.multiple_of(me * 64, 64), 64), :] = wsend_gu[e, me]

    def send_gu(e):
        def send(dst):
            remote(
                wsend_gu.at[e, dst], wgu.at[e, pl.ds(pl.multiple_of(me * 64, 64), 64)], swgu.at[e], rwgu.at[e], dst, t
            ).start()

        to_peers(send)

    def cast_d(e):
        loads[0 if e == 0 else 6].wait()

        def block(b):
            rows = pl.ds(b * 4, 4)
            wsend_d[e, rows] = dbuf[e, rows].astype(BF16)

        loop(8, block)
        wd[e, pl.ds(pl.multiple_of(me * 32, 32), 32), :] = wsend_d[e, me]

    def send_d(e):
        def send(dst):
            remote(
                wsend_d.at[e, dst], wd.at[e, pl.ds(pl.multiple_of(me * 32, 32), 32)], swd.at[e], rwd.at[e], dst, t
            ).start()

        to_peers(send)

    cast_d(0)
    pl.semaphore_wait(barrier, NFS - 1 + 3)
    send_d(0)

    r0, r1 = rt_ref[0:1, :], rt_ref[1:2, :]
    experts = lax.broadcasted_iota(jnp.int32, (64, 768), 0)
    oh0 = (experts == r0).astype(F32)
    oh1 = (experts == r1).astype(F32)
    before = lax.broadcasted_iota(jnp.int32, (768, 768), 0) < lax.broadcasted_iota(jnp.int32, (768, 768), 1)
    count = jnp.dot((oh0 + oh1).astype(BF16), before.astype(F32).astype(BF16), preferred_element_type=F32)
    rank0 = jnp.sum(count * oh0, axis=0, keepdims=True).astype(jnp.int32)
    rank1 = jnp.sum(count * oh1, axis=0, keepdims=True).astype(jnp.int32)
    slots[0:1, :] = r0 * CAP + rank0
    slots[1:2, :] = r1 * CAP + rank1

    loads[1].wait()

    def norm(b):
        rows = pl.ds(pl.multiple_of(b * 64, 64), 64)
        x = pbuf[rows, :].astype(F32)
        scale = lax.rsqrt(jnp.mean(x * x, axis=-1, keepdims=True) + norm_eps)
        mine = pbuf[rows, pl.ds(pl.multiple_of(t * 256, 256), 256)].astype(F32)
        nm[rows, :] = (mine * scale).astype(BF16)

    loop(12, norm)

    def build(i):
        z = (mz + plane_step(i)) % NZ
        index = lax.broadcasted_iota(jnp.int32, (8 * CAP, 768), 0) + z * (8 * CAP)
        hit = (index == slots[0:1, :]) | (index == slots[1:2, :])
        rows = jnp.dot(hit.astype(F32).astype(BF16), nm[...], preferred_element_type=F32)
        outbox[pl.ds(z * 8, 8)] = rows.astype(BF16).reshape(8, CAP, 256)

    def send_t(i):
        z = (mz + plane_step(i)) % NZ
        for dy in range(NY):
            dst = z * NY + (my + dy) % NY

            def go(dst=dst):
                remote(outbox.at[pl.ds(dst * 2, 2)], tok.at[t, me], st, own.at[i], dst, t).start()

            if dy == 0:
                pl.when(i > 0)(go)
            else:
                go()

    def dispatch(i):
        build(i)

        @pl.when(i > 0)
        def _():
            send_t(i - 1)

    loop(NZ, dispatch)
    tok[t, me] = outbox[pl.ds(me * 2, 2)]
    cast_gu(0)
    send_t(NZ - 1)
    send_gu(0)
    cast_gu(1)
    cast_d(1)
    send_gu(1)
    send_d(1)

    def plane_rows(i):
        z = (mz + 2 * NZ - plane_step(i)) % NZ
        return z * NY

    def gather(i):
        @pl.when(i < NZ)
        def _():
            at = plane_rows(i)

            @pl.when(i > 0)
            def _():
                got(tok.at[t, pl.ds(at, NY)], own.at[i])

            @pl.when(i == 0)
            def _():
                got(tok.at[t, pl.ds(at, NY - 1)], own.at[i])

            piece = tok.at[t, pl.ds(at, NY)]
            remote(piece, piece, sx, xl.at[i], me, right).start()
            remote(piece, piece, sx, xr.at[i], me, left).start()
            remote(piece, piece, sx, po.at[i], me, mate).start()

        @pl.when((i >= 1) & (i < NZ + 1))
        def _():
            j = i - 1
            at = plane_rows(j)
            whole = tok.at[left, pl.ds(at, NY)]
            half = tok.at[left, pl.ds(at, NY // 2)]
            got(whole, xl.at[j])
            remote(half, half, sx, fl.at[j], me, right).start()
            remote(whole, whole, sx, pl_.at[j], me, mate).start()
            whole = tok.at[right, pl.ds(at, NY)]
            half = tok.at[right, pl.ds(at + NY // 2, NY // 2)]
            got(whole, xr.at[j])
            remote(half, half, sx, fr.at[j], me, left).start()
            remote(whole, whole, sx, pr.at[j], me, mate).start()

        @pl.when(i >= 2)
        def _():
            j = i - 2
            at = plane_rows(j)
            whole = tok.at[far, pl.ds(at, NY)]
            got(tok.at[far, pl.ds(at, NY // 2)], fl.at[j])
            got(tok.at[far, pl.ds(at + NY // 2, NY // 2)], fr.at[j])
            remote(whole, whole, sx, pf.at[j], me, mate).start()

    loop(NZ + 2, gather)

    def gathered(i):
        at = pl.ds(plane_rows(i), NY)
        got(tok.at[mate, at], po.at[i])
        got(tok.at[left + 1 - 2 * mc, at], pl_.at[i])
        got(tok.at[right + 1 - 2 * mc, at], pr.at[i])
        got(tok.at[far + 1 - 2 * mc, at], pf.at[i])

    loop(NZ, gathered)

    CH = 8
    NCH = NFS // CH
    CR = CH * CAP

    def chunk_of(k):
        step = (2 + ((k + 1) // 2) * (1 - 2 * (k % 2))) % NCH
        return (mz // 2 + step) % NCH

    def expert(e):
        got(wsend_gu.at[e, pl.ds(0, NFS - 1)], rwgu.at[e])
        pltpu.make_async_copy(wgu.at[e, :, pl.ds(0, 128)], gate_out.at[e], out_sem.at[3 * e]).start()
        pltpu.make_async_copy(wgu.at[e, :, pl.ds(128, 128)], up_out.at[e], out_sem.at[3 * e + 1]).start()

        def hrows(k):
            return pl.ds(pl.multiple_of(chunk_of(k) * CR, CR), CR)

        def send_h(k):
            piece = hid.at[t, e, hrows(k)]
            remote(piece, piece, sh.at[e], hxl.at[e, k], me, right).start()
            remote(piece, piece, sh.at[e], hxr.at[e, k], me, left).start()
            remote(piece, piece, sh.at[e], hpo.at[e, k], me, mate).start()

        def forward_h(k):
            base = pl.multiple_of(chunk_of(k) * CR, CR)
            whole = hid.at[left, e, pl.ds(base, CR)]
            half = hid.at[left, e, pl.ds(base, CR // 2)]
            got(whole, hxl.at[e, k])
            remote(half, half, sh.at[e], hfl.at[e, k], me, right).start()
            remote(whole, whole, sh.at[e], hpl.at[e, k], me, mate).start()
            whole = hid.at[right, e, pl.ds(base, CR)]
            half = hid.at[right, e, pl.ds(base + CR // 2, CR // 2)]
            got(whole, hxr.at[e, k])
            remote(half, half, sh.at[e], hfr.at[e, k], me, left).start()
            remote(whole, whole, sh.at[e], hpr.at[e, k], me, mate).start()

        def pass_h(k):
            base = pl.multiple_of(chunk_of(k) * CR, CR)
            whole = hid.at[far, e, pl.ds(base, CR)]
            got(hid.at[far, e, pl.ds(base, CR // 2)], hfl.at[e, k])
            got(hid.at[far, e, pl.ds(base + CR // 2, CR // 2)], hfr.at[e, k])
            remote(whole, whole, sh.at[e], hpf.at[e, k], me, mate).start()

        def up_step(k):
            @pl.when(k < NCH)
            def _():
                senders = pl.ds(chunk_of(k) * CH, CH)
                acc = jnp.zeros((CR, 256), F32)
                for p in range(NTP):
                    x = tok[p, senders, e].reshape(CR, 256)
                    acc = acc + jnp.dot(x, wgu[e, p * 256 : (p + 1) * 256, :], preferred_element_type=F32)
                gate, up = acc[:, 0:128], acc[:, 128:256]
                hid[t, e, hrows(k), :] = (gate / (1.0 + jnp.exp(-gate)) * up).astype(BF16)

            @pl.when((k >= 1) & (k < NCH + 1))
            def _():
                send_h(k - 1)

            @pl.when((k >= 2) & (k < NCH + 2))
            def _():
                forward_h(k - 2)

            @pl.when(k >= 3)
            def _():
                pass_h(k - 3)

        loop(NCH + 3, up_step)

        got(wsend_d.at[e, pl.ds(0, NFS - 1)], rwd.at[e])
        pltpu.make_async_copy(wd.at[e], down_out.at[e], out_sem.at[3 * e + 2]).start()

        def send_r(k):
            plane = chunk_of(k) * 2
            for n in range(CH):
                s = (plane + n // NY) * NY + (my + n) % NY

                def go(s=s):
                    remote(eo.at[e, s], ret.at[e, me], sr.at[e], rr.at[e], s, t).start()

                if n % NY == 0:
                    pl.when(s != me)(go)
                else:
                    go()

        def down_step(k):
            @pl.when(k < NCH)
            def _():
                rows = hrows(k)
                got(hid.at[mate, e, rows], hpo.at[e, k])
                got(hid.at[left + 1 - 2 * mc, e, rows], hpl.at[e, k])
                got(hid.at[right + 1 - 2 * mc, e, rows], hpr.at[e, k])
                got(hid.at[far + 1 - 2 * mc, e, rows], hpf.at[e, k])
                acc = jnp.zeros((CR, 256), F32)
                for q in range(NX):
                    h = jnp.concatenate([hid[2 * q, e, rows, :], hid[2 * q + 1, e, rows, :]], axis=1)
                    acc = acc + jnp.dot(h, wd[e, q * 256 : (q + 1) * 256, :], preferred_element_type=F32)
                eo[e, pl.ds(chunk_of(k) * CH, CH)] = acc.astype(BF16).reshape(CH, CAP, 256)

            @pl.when(k >= 1)
            def _():
                send_r(k - 1)

        loop(NCH + 1, down_step)
        ret[e, me] = eo[e, me]

    expert(0)
    expert(1)

    r0, r1 = rt_ref[0:1, :], rt_ref[1:2, :]
    rank0, rank1 = slots[0:1, :] - r0 * CAP, slots[1:2, :] - r1 * CAP
    a0, a1 = at_ref[0:1, :], at_ref[1:2, :]
    total = a0 + a1

    def keys(r, rank, e):
        key = jnp.right_shift(r, 1) * CAP + rank
        return jnp.where(jnp.bitwise_and(r, 1) == e, key, -1).astype(F32)

    packed = jnp.concatenate(
        [keys(r0, rank0, 0), keys(r1, rank1, 0), keys(r0, rank0, 1), keys(r1, rank1, 1), a0 / total, a1 / total,
         jnp.zeros((122, 768), F32)],
        axis=0,
    )
    macc[...] = jnp.concatenate([packed.T, jnp.zeros((768, 128), F32)], axis=1)

    def weigh(b):
        rows = pl.ds(pl.multiple_of(b * 64, 64), 64)
        columns = macc[rows, 0:128]
        index = lax.broadcasted_iota(jnp.int32, (64, NFS * CAP), 1).astype(F32)
        for e in range(2):
            first = jnp.where(index == columns[:, 2 * e : 2 * e + 1], columns[:, 4:5], 0.0)
            second = jnp.where(index == columns[:, 2 * e + 1 : 2 * e + 2], columns[:, 5:6], 0.0)
            wcomb[e, rows, :] = (first + second).astype(BF16)

    loop(12, weigh)

    got(ret.at[0, pl.ds(0, NFS - 1)], rr.at[0])

    def mix_first(b):
        rows = pl.ds(pl.multiple_of(b * 256, 256), 256)
        macc[rows, :] = jnp.dot(wcomb[0, rows, :], ret[0].reshape(NFS * CAP, 256), preferred_element_type=F32)

    loop(3, mix_first)
    got(ret.at[1, pl.ds(0, NFS - 1)], rr.at[1])

    def mix_second(b):
        rows = pl.ds(pl.multiple_of(b * 256, 256), 256)
        both = macc[rows, :] + jnp.dot(wcomb[1, rows, :], ret[1].reshape(NFS * CAP, 256), preferred_element_type=F32)
        mixed_ref[rows, :] = both.astype(BF16)

    loop(3, mix_second)

    for e in range(2):
        sent(wsend_gu.at[e, pl.ds(0, NFS - 1)], swgu.at[e])
        sent(wsend_d.at[e, pl.ds(0, NFS - 1)], swd.at[e])
        sent(hid.at[pl.ds(0, 7), e], sh.at[e])
        sent(eo.at[e, pl.ds(0, NFS - 1)], sr.at[e])
        pltpu.make_async_copy(wgu.at[e, :, pl.ds(0, 128)], gate_out.at[e], out_sem.at[3 * e]).wait()
        pltpu.make_async_copy(wgu.at[e, :, pl.ds(128, 128)], up_out.at[e], out_sem.at[3 * e + 1]).wait()
        pltpu.make_async_copy(wd.at[e], down_out.at[e], out_sem.at[3 * e + 2]).wait()
    sent(outbox.at[pl.ds(0, 2 * (NFS - 1))], st)
    sent(tok.at[pl.ds(0, 7)], sx)


def per_device(prompt, routes, affinity, norm_gain, gate_master, up_master, down_master):
    vmem = pl.BlockSpec(memory_space=pltpu.VMEM)
    hbm = pl.BlockSpec(memory_space=pl.ANY)
    dma = pltpu.SemaphoreType.DMA
    scratch = [
        pltpu.VMEM((768, 2048), BF16),
        pltpu.VMEM((2, 32, 64, 128), F32),
        pltpu.VMEM((2, 32, 64, 128), F32),
        pltpu.VMEM((2, 32, 32, 256), F32),
        pltpu.VMEM((2, 32, 64, 256), BF16),
        pltpu.VMEM((2, 32, 32, 256), BF16),
        pltpu.VMEM((768, 256), BF16),
        pltpu.VMEM((64, CAP, 256), BF16),
        pltpu.VMEM((NTP, NFS, 2, CAP, 256), BF16),
        pltpu.VMEM((2, 2048, 256), BF16),
        pltpu.VMEM((2, 1024, 256), BF16),
        pltpu.VMEM((NTP, 2, NFS * CAP, 128), BF16),
        pltpu.VMEM((2, NFS, CAP, 256), BF16),
        pltpu.VMEM((2, NFS, CAP, 256), BF16),
        pltpu.VMEM((2, 768, NFS * CAP), BF16),
        pltpu.VMEM((768, 256), F32),
        pltpu.VMEM((8, 768), jnp.int32),
        dma((7,)),
        dma((6,)),
        dma((2,)), dma((2,)), dma((2,)), dma((2,)),
        dma, dma,
        *[dma((NZ,)) for _ in range(9)],
        dma((2,)),
        *[dma((2, 4)) for _ in range(8)],
        dma((2,)), dma((2,)),
    ]
    return pl.pallas_call(
        kernel,
        out_shape=(
            jax.ShapeDtypeStruct((768, 256), BF16),
            jax.ShapeDtypeStruct((2, 2048, 128), BF16),
            jax.ShapeDtypeStruct((2, 2048, 128), BF16),
            jax.ShapeDtypeStruct((2, 1024, 256), BF16),
        ),
        in_specs=[vmem] * 3 + [hbm] * 4,
        out_specs=(vmem, hbm, hbm, hbm),
        scratch_shapes=scratch,
        compiler_params=pltpu.CompilerParams(
            collective_id=0, has_side_effects=True, vmem_limit_bytes=60 * 1024 * 1024
        ),
        name="hand_off",
    )(
        routes.T,
        affinity.T,
        jnp.broadcast_to(norm_gain[:, None], (64, 128)),
        prompt,
        gate_master.reshape(32, 2, 64, 128),
        up_master.reshape(32, 2, 64, 128),
        down_master.reshape(32, 2, 32, 256),
    )


def solution(mesh):
    in_specs = (
        P("fs", None),
        P("fs", None),
        P("fs", None),
        P("fs"),
        P(None, "fs", "tp"),
        P(None, "fs", "tp"),
        P(None, "fs", "tp"),
    )
    out_specs = (P("fs", "tp"), P("fs", None, "tp"), P("fs", None, "tp"), P("fs", None, "tp"))
    return jax.shard_map(
        per_device, mesh=mesh, in_specs=in_specs, out_specs=out_specs, check_vma=False
    )
```

```python
import jax
import jax.numpy as jnp
from jax import lax
from jax.experimental import pallas as pl
from jax.experimental.pallas import tpu as pltpu
from jax.sharding import PartitionSpec as P

MESH = pl.DeviceIdType.MESH
norm_eps = 1e-06

NZ, NY, NX = 8, 4, 4
NFS = NZ * NY
NTP = NX * 2
CAP = 48
BF16, F32 = jnp.bfloat16, jnp.float32


def plane_step(i):
    return NZ + ((i + 1) // 2) * (2 * (i % 2) - 1)


def loop(count, body):
    def step(i, carry):
        body(i)
        return carry

    lax.fori_loop(0, count, step, 0)


def kernel(
    rt_hbm, at_hbm, gain_hbm, prompt_ref, gate_ref, up_ref, down_ref,
    wgu, wd, macc, wcomb1, ret1,
    rt_ref, at_ref, gain_ref, pbuf, gbuf, ubuf, dbuf, wsend_gu, wsend_d, nm, outbox, tok, hid, eo, ret0, wcomb0,
    slots, load_sem, swgu, swd, rwgu, rwd, st, sx, own, xl, xr, fl, fr, po, pl_, pr, pf,
    sh, hxl, hxr, hfl, hfr, hpo, hpl, hpr, hpf, sr, rr,
):
    me = lax.axis_index("fs")
    t = lax.axis_index("tp")
    mz, my = me // NY, me % NY
    mx, mc = t // 2, t % 2
    right = ((mx + 1) % NX) * 2 + mc
    left = ((mx + NX - 1) % NX) * 2 + mc
    far = ((mx + 2) % NX) * 2 + mc
    mate = mx * 2 + 1 - mc

    ret, wcomb = (ret0, ret1), (wcomb0, wcomb1)

    def load(n, src, dst):
        return pltpu.make_async_copy(src, dst, load_sem.at[n])

    loads = [
        load(3, down_ref.at[:, 0], dbuf.at[0]),
        load(2, prompt_ref, pbuf),
        load(0, gate_ref.at[:, 0], gbuf.at[0]),
        load(1, up_ref.at[:, 0], ubuf.at[0]),
        load(4, gate_ref.at[:, 1], gbuf.at[1]),
        load(5, up_ref.at[:, 1], ubuf.at[1]),
        load(6, down_ref.at[:, 1], dbuf.at[1]),
        load(7, rt_hbm, rt_ref),
        load(8, at_hbm, at_ref),
        load(9, gain_hbm, gain_ref),
    ]
    for n in (0, 7, 1, 9, 2, 3, 4, 5, 6, 8):
        loads[n].start()

    barrier = pltpu.get_barrier_semaphore()

    def greet(i):
        pl.semaphore_signal(barrier, inc=1, device_id=((me + 1 + i) % NFS, t), device_id_type=MESH)

    loop(NFS - 1, greet)
    for other in (right, left, mate):
        pl.semaphore_signal(barrier, inc=1, device_id=(me, other), device_id_type=MESH)

    def remote(src, dst, ssem, rsem, fs, tp):
        return pltpu.make_async_remote_copy(
            src_ref=src, dst_ref=dst, send_sem=ssem, recv_sem=rsem, device_id=(fs, tp), device_id_type=MESH
        )

    def got(ref, sem):
        remote(ref, ref, sem, sem, me, t).wait_recv()

    def sent(ref, sem):
        remote(ref, ref, sem, sem, me, t).wait_send()

    def to_peers(send):
        def plane(i):
            z = (mz + plane_step(i)) % NZ
            for dy in range(NY):
                dst = z * NY + (my + dy) % NY
                if dy == 0:
                    @pl.when(i > 0)
                    def _():
                        send(dst)
                else:
                    send(dst)

        loop(NZ, plane)

    def cast_gu(e):
        if e == 0:
            loads[9].wait()
        loads[2 if e == 0 else 4].wait()
        loads[3 if e == 0 else 5].wait()

        diagonal = lax.broadcasted_iota(jnp.int32, (64, 64), 0) == lax.broadcasted_iota(jnp.int32, (64, 64), 1)
        column = jnp.sum(jnp.where(diagonal, gain_ref[...], 0.0), axis=1, keepdims=True)
        gain = jnp.broadcast_to(column, (64, 128))[None]

        def block(b):
            rows = pl.ds(b * 4, 4)
            wsend_gu[e, rows, :, 0:128] = (gbuf[e, rows] * gain).astype(BF16)
            wsend_gu[e, rows, :, 128:256] = (ubuf[e, rows] * gain).astype(BF16)

        loop(8, block)
        wgu[e, pl.ds(pl.multiple_of(me * 64, 64), 64), :] = wsend_gu[e, me]

    def send_gu(e):
        def send(dst):
            remote(
                wsend_gu.at[e, dst], wgu.at[e, pl.ds(pl.multiple_of(me * 64, 64), 64)], swgu.at[e], rwgu.at[e], dst, t
            ).start()

        to_peers(send)

    def cast_d(e):
        loads[0 if e == 0 else 6].wait()

        def block(b):
            rows = pl.ds(b * 4, 4)
            wsend_d[e, rows] = dbuf[e, rows].astype(BF16)

        loop(8, block)
        wd[e, pl.ds(pl.multiple_of(me * 32, 32), 32), :] = wsend_d[e, me]

    def send_d(e):
        def send(dst):
            remote(
                wsend_d.at[e, dst], wd.at[e, pl.ds(pl.multiple_of(me * 32, 32), 32)], swd.at[e], rwd.at[e], dst, t
            ).start()

        to_peers(send)

    cast_d(0)
    pl.semaphore_wait(barrier, NFS - 1 + 3)
    send_d(0)

    loads[7].wait()
    r0, r1 = rt_ref[0:1, :], rt_ref[1:2, :]
    experts = lax.broadcasted_iota(jnp.int32, (64, 768), 0)
    oh0 = (experts == r0).astype(F32)
    oh1 = (experts == r1).astype(F32)
    before = lax.broadcasted_iota(jnp.int32, (768, 768), 0) < lax.broadcasted_iota(jnp.int32, (768, 768), 1)
    count = jnp.dot((oh0 + oh1).astype(BF16), before.astype(F32).astype(BF16), preferred_element_type=F32)
    rank0 = jnp.sum(count * oh0, axis=0, keepdims=True).astype(jnp.int32)
    rank1 = jnp.sum(count * oh1, axis=0, keepdims=True).astype(jnp.int32)
    slots[0:1, :] = r0 * CAP + rank0
    slots[1:2, :] = r1 * CAP + rank1

    loads[1].wait()

    def norm(b):
        rows = pl.ds(pl.multiple_of(b * 64, 64), 64)
        x = pbuf[rows, :].astype(F32)
        scale = lax.rsqrt(jnp.mean(x * x, axis=-1, keepdims=True) + norm_eps)
        mine = pbuf[rows, pl.ds(pl.multiple_of(t * 256, 256), 256)].astype(F32)
        nm[rows, :] = (mine * scale).astype(BF16)

    loop(12, norm)

    def build(i):
        z = (mz + plane_step(i)) % NZ
        index = lax.broadcasted_iota(jnp.int32, (8 * CAP, 768), 0) + z * (8 * CAP)
        hit = (index == slots[0:1, :]) | (index == slots[1:2, :])
        rows = jnp.dot(hit.astype(F32).astype(BF16), nm[...], preferred_element_type=F32)
        outbox[pl.ds(z * 8, 8)] = rows.astype(BF16).reshape(8, CAP, 256)

    def send_t(i):
        z = (mz + plane_step(i)) % NZ
        for dy in range(NY):
            dst = z * NY + (my + dy) % NY

            def go(dst=dst):
                remote(outbox.at[pl.ds(dst * 2, 2)], tok.at[t, me], st, own.at[i], dst, t).start()

            if dy == 0:
                pl.when(i > 0)(go)
            else:
                go()

    def dispatch(i):
        build(i)

        @pl.when(i > 0)
        def _():
            send_t(i - 1)

    loop(NZ, dispatch)
    tok[t, me] = outbox[pl.ds(me * 2, 2)]
    cast_gu(0)
    send_t(NZ - 1)
    send_gu(0)
    cast_gu(1)
    cast_d(1)
    send_gu(1)
    send_d(1)

    def plane_rows(i):
        z = (mz + 2 * NZ - plane_step(i)) % NZ
        return z * NY

    def gather(i):
        @pl.when(i < NZ)
        def _():
            at = plane_rows(i)

            @pl.when(i > 0)
            def _():
                got(tok.at[t, pl.ds(at, NY)], own.at[i])

            @pl.when(i == 0)
            def _():
                got(tok.at[t, pl.ds(at, NY - 1)], own.at[i])

            piece = tok.at[t, pl.ds(at, NY)]
            remote(piece, piece, sx, xl.at[i], me, right).start()
            remote(piece, piece, sx, xr.at[i], me, left).start()
            remote(piece, piece, sx, po.at[i], me, mate).start()

        @pl.when((i >= 1) & (i < NZ + 1))
        def _():
            j = i - 1
            at = plane_rows(j)
            whole = tok.at[left, pl.ds(at, NY)]
            half = tok.at[left, pl.ds(at, NY // 2)]
            got(whole, xl.at[j])
            remote(half, half, sx, fl.at[j], me, right).start()
            remote(whole, whole, sx, pl_.at[j], me, mate).start()
            whole = tok.at[right, pl.ds(at, NY)]
            half = tok.at[right, pl.ds(at + NY // 2, NY // 2)]
            got(whole, xr.at[j])
            remote(half, half, sx, fr.at[j], me, left).start()
            remote(whole, whole, sx, pr.at[j], me, mate).start()

        @pl.when(i >= 2)
        def _():
            j = i - 2
            at = plane_rows(j)
            whole = tok.at[far, pl.ds(at, NY)]
            got(tok.at[far, pl.ds(at, NY // 2)], fl.at[j])
            got(tok.at[far, pl.ds(at + NY // 2, NY // 2)], fr.at[j])
            remote(whole, whole, sx, pf.at[j], me, mate).start()

    loop(NZ + 2, gather)

    def gathered(i):
        at = pl.ds(plane_rows(i), NY)
        got(tok.at[mate, at], po.at[i])
        got(tok.at[left + 1 - 2 * mc, at], pl_.at[i])
        got(tok.at[right + 1 - 2 * mc, at], pr.at[i])
        got(tok.at[far + 1 - 2 * mc, at], pf.at[i])

    loop(NZ, gathered)

    CH = 8
    NCH = NFS // CH
    CR = CH * CAP

    def chunk_of(k):
        step = (2 + ((k + 1) // 2) * (1 - 2 * (k % 2))) % NCH
        return (mz // 2 + step) % NCH

    def expert(e):
        got(wsend_gu.at[e, pl.ds(0, NFS - 1)], rwgu.at[e])

        def hrows(k):
            return pl.ds(pl.multiple_of(chunk_of(k) * CR, CR), CR)

        def send_h(k):
            piece = hid.at[t, e, hrows(k)]
            remote(piece, piece, sh.at[e], hxl.at[e, k], me, right).start()
            remote(piece, piece, sh.at[e], hxr.at[e, k], me, left).start()
            remote(piece, piece, sh.at[e], hpo.at[e, k], me, mate).start()

        def forward_h(k):
            base = pl.multiple_of(chunk_of(k) * CR, CR)
            whole = hid.at[left, e, pl.ds(base, CR)]
            half = hid.at[left, e, pl.ds(base, CR // 2)]
            got(whole, hxl.at[e, k])
            remote(half, half, sh.at[e], hfl.at[e, k], me, right).start()
            remote(whole, whole, sh.at[e], hpl.at[e, k], me, mate).start()
            whole = hid.at[right, e, pl.ds(base, CR)]
            half = hid.at[right, e, pl.ds(base + CR // 2, CR // 2)]
            got(whole, hxr.at[e, k])
            remote(half, half, sh.at[e], hfr.at[e, k], me, left).start()
            remote(whole, whole, sh.at[e], hpr.at[e, k], me, mate).start()

        def pass_h(k):
            base = pl.multiple_of(chunk_of(k) * CR, CR)
            whole = hid.at[far, e, pl.ds(base, CR)]
            got(hid.at[far, e, pl.ds(base, CR // 2)], hfl.at[e, k])
            got(hid.at[far, e, pl.ds(base + CR // 2, CR // 2)], hfr.at[e, k])
            remote(whole, whole, sh.at[e], hpf.at[e, k], me, mate).start()

        def up_step(k):
            @pl.when(k < NCH)
            def _():
                senders = pl.ds(chunk_of(k) * CH, CH)
                acc = jnp.zeros((CR, 256), F32)
                for p in range(NTP):
                    x = tok[p, senders, e].reshape(CR, 256)
                    acc = acc + jnp.dot(x, wgu[e, p * 256 : (p + 1) * 256, :], preferred_element_type=F32)
                gate, up = acc[:, 0:128], acc[:, 128:256]
                hid[t, e, hrows(k), :] = (gate / (1.0 + jnp.exp(-gate)) * up).astype(BF16)

            @pl.when((k >= 1) & (k < NCH + 1))
            def _():
                send_h(k - 1)

            @pl.when((k >= 2) & (k < NCH + 2))
            def _():
                forward_h(k - 2)

            @pl.when(k >= 3)
            def _():
                pass_h(k - 3)

        loop(NCH + 3, up_step)

        got(wsend_d.at[e, pl.ds(0, NFS - 1)], rwd.at[e])

        def send_r(k):
            plane = chunk_of(k) * 2
            for n in range(CH):
                s = (plane + n // NY) * NY + (my + n) % NY

                def go(s=s):
                    remote(eo.at[e, s], ret[e].at[me], sr.at[e], rr.at[e], s, t).start()

                if n % NY == 0:
                    pl.when(s != me)(go)
                else:
                    go()

        def down_step(k):
            @pl.when(k < NCH)
            def _():
                rows = hrows(k)
                got(hid.at[mate, e, rows], hpo.at[e, k])
                got(hid.at[left + 1 - 2 * mc, e, rows], hpl.at[e, k])
                got(hid.at[right + 1 - 2 * mc, e, rows], hpr.at[e, k])
                got(hid.at[far + 1 - 2 * mc, e, rows], hpf.at[e, k])
                acc = jnp.zeros((CR, 256), F32)
                for q in range(NX):
                    h = jnp.concatenate([hid[2 * q, e, rows, :], hid[2 * q + 1, e, rows, :]], axis=1)
                    acc = acc + jnp.dot(h, wd[e, q * 256 : (q + 1) * 256, :], preferred_element_type=F32)
                eo[e, pl.ds(chunk_of(k) * CH, CH)] = acc.astype(BF16).reshape(CH, CAP, 256)

            @pl.when(k >= 1)
            def _():
                send_r(k - 1)

        loop(NCH + 1, down_step)
        ret[e][me] = eo[e, me]

    expert(0)
    expert(1)

    r0, r1 = rt_ref[0:1, :], rt_ref[1:2, :]
    rank0, rank1 = slots[0:1, :] - r0 * CAP, slots[1:2, :] - r1 * CAP
    loads[8].wait()
    a0, a1 = at_ref[0:1, :], at_ref[1:2, :]
    total = a0 + a1

    def keys(r, rank, e):
        key = jnp.right_shift(r, 1) * CAP + rank
        return jnp.where(jnp.bitwise_and(r, 1) == e, key, -1).astype(F32)

    packed = jnp.concatenate(
        [keys(r0, rank0, 0), keys(r1, rank1, 0), keys(r0, rank0, 1), keys(r1, rank1, 1), a0 / total, a1 / total,
         jnp.zeros((122, 768), F32)],
        axis=0,
    )
    macc[...] = jnp.concatenate([packed.T, jnp.zeros((768, 128), F32)], axis=1)

    def weigh(b):
        rows = pl.ds(pl.multiple_of(b * 64, 64), 64)
        columns = macc[rows, 0:128]
        index = lax.broadcasted_iota(jnp.int32, (64, NFS * CAP), 1).astype(F32)
        for e in range(2):
            first = jnp.where(index == columns[:, 2 * e : 2 * e + 1], columns[:, 4:5], 0.0)
            second = jnp.where(index == columns[:, 2 * e + 1 : 2 * e + 2], columns[:, 5:6], 0.0)
            wcomb[e][rows, :] = (first + second).astype(BF16)

    loop(12, weigh)

    got(ret0.at[pl.ds(0, NFS - 1)], rr.at[0])

    def mix_first(b):
        rows = pl.ds(pl.multiple_of(b * 256, 256), 256)
        macc[rows, :] = jnp.dot(wcomb0[rows, :], ret0[...].reshape(NFS * CAP, 256), preferred_element_type=F32)

    loop(3, mix_first)
    got(ret1.at[pl.ds(0, NFS - 1)], rr.at[1])

    for e in range(2):
        sent(wsend_gu.at[e, pl.ds(0, NFS - 1)], swgu.at[e])
        sent(wsend_d.at[e, pl.ds(0, NFS - 1)], swd.at[e])
        sent(hid.at[pl.ds(0, 7), e], sh.at[e])
        sent(eo.at[e, pl.ds(0, NFS - 1)], sr.at[e])
    sent(outbox.at[pl.ds(0, 2 * (NFS - 1))], st)
    sent(tok.at[pl.ds(0, 7)], sx)


def finish(wgu, wd, macc, wcomb1, ret1, mixed_out, gate_out, up_out, down_out, mixed, sem):
    copies = [
        pltpu.make_async_copy(wgu.at[:, :, pl.ds(0, 128)], gate_out, sem.at[0]),
        pltpu.make_async_copy(wgu.at[:, :, pl.ds(128, 128)], up_out, sem.at[1]),
        pltpu.make_async_copy(wd, down_out, sem.at[2]),
    ]
    for c in copies:
        c.start()
    for b in range(3):
        rows = pl.ds(b * 256, 256)
        odd = jnp.dot(wcomb1[rows, :], ret1[...].reshape(NFS * CAP, 256), preferred_element_type=F32)
        mixed[rows, :] = (macc[rows, :] + odd).astype(BF16)
    last = pltpu.make_async_copy(mixed, mixed_out, sem.at[3])
    last.start()
    for c in copies + [last]:
        c.wait()


def per_device(prompt, routes, affinity, norm_gain, gate_master, up_master, down_master):
    vmem = pl.BlockSpec(memory_space=pltpu.VMEM)
    hbm = pl.BlockSpec(memory_space=pl.ANY)
    dma = pltpu.SemaphoreType.DMA
    scratch = [
        pltpu.VMEM((2, 768), jnp.int32),
        pltpu.VMEM((2, 768), F32),
        pltpu.VMEM((1, 64), F32),
        pltpu.VMEM((768, 2048), BF16),
        pltpu.VMEM((2, 32, 64, 128), F32),
        pltpu.VMEM((2, 32, 64, 128), F32),
        pltpu.VMEM((2, 32, 32, 256), F32),
        pltpu.VMEM((2, 32, 64, 256), BF16),
        pltpu.VMEM((2, 32, 32, 256), BF16),
        pltpu.VMEM((768, 256), BF16),
        pltpu.VMEM((64, CAP, 256), BF16),
        pltpu.VMEM((NTP, NFS, 2, CAP, 256), BF16),
        pltpu.VMEM((NTP, 2, NFS * CAP, 128), BF16),
        pltpu.VMEM((2, NFS, CAP, 256), BF16),
        pltpu.VMEM((NFS, CAP, 256), BF16),
        pltpu.VMEM((768, NFS * CAP), BF16),
        pltpu.VMEM((8, 768), jnp.int32),
        dma((10,)),
        dma((2,)), dma((2,)), dma((2,)), dma((2,)),
        dma, dma,
        *[dma((NZ,)) for _ in range(9)],
        dma((2,)),
        *[dma((2, 4)) for _ in range(8)],
        dma((2,)), dma((2,)),
    ]
    landed = pl.pallas_call(
        kernel,
        out_shape=(
            pltpu.VMEM((2, 2048, 256), BF16),
            pltpu.VMEM((2, 1024, 256), BF16),
            pltpu.VMEM((768, 256), F32),
            pltpu.VMEM((768, NFS * CAP), BF16),
            pltpu.VMEM((NFS, CAP, 256), BF16),
        ),
        in_specs=[hbm] * 7,
        out_specs=(vmem,) * 5,
        scratch_shapes=scratch,
        compiler_params=pltpu.CompilerParams(
            collective_id=0, has_side_effects=True, vmem_limit_bytes=50 * 1024 * 1024
        ),
        name="hand_off",
    )(
        routes.T,
        affinity.T,
        norm_gain.reshape(1, 64),
        prompt,
        gate_master.reshape(32, 2, 64, 128),
        up_master.reshape(32, 2, 64, 128),
        down_master.reshape(32, 2, 32, 256),
    )
    return pl.pallas_call(
        finish,
        out_shape=(
            jax.ShapeDtypeStruct((768, 256), BF16),
            jax.ShapeDtypeStruct((2, 2048, 128), BF16),
            jax.ShapeDtypeStruct((2, 2048, 128), BF16),
            jax.ShapeDtypeStruct((2, 1024, 256), BF16),
        ),
        in_specs=[vmem] * 5,
        out_specs=(hbm,) * 4,
        scratch_shapes=[pltpu.VMEM((768, 256), BF16), dma((4,))],
        compiler_params=pltpu.CompilerParams(vmem_limit_bytes=8 * 1024 * 1024),
        name="finish",
    )(*landed)


def solution(mesh):
    in_specs = (
        P("fs", None),
        P("fs", None),
        P("fs", None),
        P("fs"),
        P(None, "fs", "tp"),
        P(None, "fs", "tp"),
        P(None, "fs", "tp"),
    )
    out_specs = (P("fs", "tp"), P("fs", None, "tp"), P("fs", None, "tp"), P("fs", None, "tp"))
    return jax.shard_map(
        per_device, mesh=mesh, in_specs=in_specs, out_specs=out_specs, check_vma=False
    )
```

```python
import jax
import jax.numpy as jnp
from jax import lax
from jax.experimental import pallas as pl
from jax.experimental.pallas import tpu as pltpu
from jax.sharding import PartitionSpec as P

MESH = pl.DeviceIdType.MESH
norm_eps = 1e-06

NZ, NY, NX = 8, 4, 4
NFS = NZ * NY
NTP = NX * 2
CAP = 48
BF16, F32 = jnp.bfloat16, jnp.float32


def plane_step(i):
    return NZ + ((i + 1) // 2) * (2 * (i % 2) - 1)


def loop(count, body, start=0):
    def step(i, carry):
        body(i)
        return carry

    lax.fori_loop(start, count, step, 0)


def kernel(
    rt_hbm, at_hbm, gain_hbm, prompt_ref, gate_ref, up_ref, down_ref,
    wgu, wd, macc, wcomb1, ret1,
    rt_ref, at_ref, gain_ref, pbuf, gbuf, ubuf, dbuf, wsend_gu, wsend_d, nm, blk, near, outbox, tok, hid, eo, ret0, wcomb0,
    slots, load_sem, sa, rblk, rnear, swgu, swd, rwgu, rwd, st, sx, own, xl, xr, fl, fr, po, pl_, pr, pf,
    sh, hxl, hxr, hfl, hfr, hpo, hpl, hpr, hpf, sr, rr,
):
    me = lax.axis_index("fs")
    t = lax.axis_index("tp")
    mz, my = me // NY, me % NY
    mx, mc = t // 2, t % 2
    right = ((mx + 1) % NX) * 2 + mc
    left = ((mx + NX - 1) % NX) * 2 + mc
    far = ((mx + 2) % NX) * 2 + mc
    mate = mx * 2 + 1 - mc

    ret, wcomb = (ret0, ret1), (wcomb0, wcomb1)

    def load(n, src, dst):
        return pltpu.make_async_copy(src, dst, load_sem.at[n])

    loads = [
        load(3, down_ref.at[:, 0], dbuf.at[0]),
        load(2, prompt_ref, pbuf),
        load(0, gate_ref.at[:, 0], gbuf.at[0]),
        load(1, up_ref.at[:, 0], ubuf.at[0]),
        load(4, gate_ref.at[:, 1], gbuf.at[1]),
        load(5, up_ref.at[:, 1], ubuf.at[1]),
        load(6, down_ref.at[:, 1], dbuf.at[1]),
        load(7, rt_hbm, rt_ref),
        load(8, at_hbm, at_ref),
        load(9, gain_hbm, gain_ref),
    ]
    for n in (1, 7, 0, 9, 2, 3, 4, 5, 6, 8):
        loads[n].start()

    barrier = pltpu.get_barrier_semaphore()

    def greet(i):
        pl.semaphore_signal(barrier, inc=1, device_id=((me + 1 + i) % NFS, t), device_id_type=MESH)

    loop(NFS - 1, greet)
    for other in (right, left, mate):
        pl.semaphore_signal(barrier, inc=1, device_id=(me, other), device_id_type=MESH)

    def remote(src, dst, ssem, rsem, fs, tp):
        return pltpu.make_async_remote_copy(
            src_ref=src, dst_ref=dst, send_sem=ssem, recv_sem=rsem, device_id=(fs, tp), device_id_type=MESH
        )

    def got(ref, sem):
        remote(ref, ref, sem, sem, me, t).wait_recv()

    def sent(ref, sem):
        remote(ref, ref, sem, sem, me, t).wait_send()

    def to_peers(send, first=0, last=NZ):
        def plane(i):
            z = (mz + plane_step(i)) % NZ
            for dy in range(NY):
                dst = z * NY + (my + dy) % NY
                if dy == 0:
                    @pl.when(i > 0)
                    def _():
                        send(dst)
                else:
                    send(dst)

        loop(last, plane, first)

    def cast_gu(e):
        if e == 0:
            loads[9].wait()
        loads[2 if e == 0 else 4].wait()
        loads[3 if e == 0 else 5].wait()

        diagonal = lax.broadcasted_iota(jnp.int32, (64, 64), 0) == lax.broadcasted_iota(jnp.int32, (64, 64), 1)
        column = jnp.sum(jnp.where(diagonal, gain_ref[...], 0.0), axis=1, keepdims=True)
        gain = jnp.broadcast_to(column, (64, 128))[None]

        def block(b):
            rows = pl.ds(b * 4, 4)
            wsend_gu[e, rows, :, 0:128] = (gbuf[e, rows] * gain).astype(BF16)
            wsend_gu[e, rows, :, 128:256] = (ubuf[e, rows] * gain).astype(BF16)

        loop(8, block)
        wgu[e, pl.ds(pl.multiple_of(me * 64, 64), 64), :] = wsend_gu[e, me]

    def send_gu(e):
        def send(dst):
            remote(
                wsend_gu.at[e, dst], wgu.at[e, pl.ds(pl.multiple_of(me * 64, 64), 64)], swgu.at[e], rwgu.at[e], dst, t
            ).start()

        to_peers(send)

    def cast_d(e):
        loads[0 if e == 0 else 6].wait()

        def block(b):
            rows = pl.ds(b * 4, 4)
            wsend_d[e, rows] = dbuf[e, rows].astype(BF16)

        loop(8, block)
        wd[e, pl.ds(pl.multiple_of(me * 32, 32), 32), :] = wsend_d[e, me]

    def send_d(e, first=0, last=NZ):
        def send(dst):
            remote(
                wsend_d.at[e, dst], wd.at[e, pl.ds(pl.multiple_of(me * 32, 32), 32)], swd.at[e], rwd.at[e], dst, t
            ).start()

        to_peers(send, first, last)

    loads[1].wait()

    def norm(b):
        rows = pl.ds(pl.multiple_of(b * 64, 64), 64)
        x = pbuf[rows, :].astype(F32)
        scale = lax.rsqrt(jnp.mean(x * x, axis=-1, keepdims=True) + norm_eps)
        mine = pbuf[rows, pl.ds(pl.multiple_of(t * 256, 256), 256)].astype(F32)
        nm[rows, :] = (mine * scale).astype(BF16)

    loop(12, norm)
    above, below = (mz + 1) % NZ * NY + my, (mz + NZ - 1) % NZ * NY + my
    pl.semaphore_wait(barrier, NFS - 1 + 3)
    remote(nm, blk.at[0], sa.at[0], rblk.at[0], above, t).start()
    remote(nm, blk.at[1], sa.at[0], rblk.at[1], below, t).start()

    loads[7].wait()
    r0, r1 = rt_ref[0:1, :], rt_ref[1:2, :]
    experts = lax.broadcasted_iota(jnp.int32, (64, 768), 0)
    oh0 = (experts == r0).astype(F32)
    oh1 = (experts == r1).astype(F32)
    before = lax.broadcasted_iota(jnp.int32, (768, 768), 0) < lax.broadcasted_iota(jnp.int32, (768, 768), 1)
    count = jnp.dot((oh0 + oh1).astype(BF16), before.astype(F32).astype(BF16), preferred_element_type=F32)
    rank0 = jnp.sum(count * oh0, axis=0, keepdims=True).astype(jnp.int32)
    rank1 = jnp.sum(count * oh1, axis=0, keepdims=True).astype(jnp.int32)
    slots[...] = jnp.concatenate([r0 * CAP + rank0, r1 * CAP + rank1, jnp.zeros((6, 768), jnp.int32)], axis=0)

    def pack(block, s0, s1, index):
        hit = (index == s0) | (index == s1)
        rows = jnp.dot(hit.astype(F32).astype(BF16), block, preferred_element_type=F32)
        return rows.astype(BF16)

    def pack_plane(block, s0, s1, z):
        index = lax.broadcasted_iota(jnp.int32, (8 * CAP, 768), 0) + z * (8 * CAP)
        return pack(block, s0, s1, index).reshape(8, CAP, 256)

    def pack_half(block, s0, s1, z, e):
        turn = lax.broadcasted_iota(jnp.int32, (4, CAP, 768), 0) * (2 * CAP)
        index = turn + lax.broadcasted_iota(jnp.int32, (4, CAP, 768), 1) + (z * (8 * CAP) + e * CAP)
        return pack(block, s0, s1, index.reshape(4 * CAP, 768)).reshape(4, CAP, 256)

    outbox[0:8] = pack_plane(nm[...], slots[0:1, :], slots[1:2, :], mz)
    remote(slots, near.at[0], sa.at[1], rnear.at[0], above, t).start()
    remote(slots, near.at[1], sa.at[1], rnear.at[1], below, t).start()
    tok[t, me] = outbox[pl.ds(my * 2, 2)]
    cast_d(0)
    for dy in range(1, NY):
        y = (my + dy) % NY
        remote(outbox.at[pl.ds(y * 2, 2)], tok.at[t, me], st, own.at[0], mz * NY + y, t).start()
    send_d(0, 0, 5)

    def plane_rows(i):
        z = (mz + 2 * NZ - plane_step(i)) % NZ
        return z * NY

    def gather(i):
        @pl.when(i < NZ)
        def _():
            at = plane_rows(i)

            @pl.when(i > 2)
            def _():
                got(tok.at[t, pl.ds(at, NY)], own.at[i])

            @pl.when(i <= 2)
            def _():
                got(tok.at[t, pl.ds(at, NY - 1)], own.at[i])

            piece = tok.at[t, pl.ds(at, NY)]
            remote(piece, piece, sx, xl.at[i], me, right).start()
            remote(piece, piece, sx, xr.at[i], me, left).start()
            remote(piece, piece, sx, po.at[i], me, mate).start()

        @pl.when((i >= 1) & (i < NZ + 1))
        def _():
            j = i - 1
            at = plane_rows(j)
            whole = tok.at[left, pl.ds(at, NY)]
            half = tok.at[left, pl.ds(at, NY // 2)]
            got(whole, xl.at[j])
            remote(half, half, sx, fl.at[j], me, right).start()
            remote(whole, whole, sx, pl_.at[j], me, mate).start()
            whole = tok.at[right, pl.ds(at, NY)]
            half = tok.at[right, pl.ds(at + NY // 2, NY // 2)]
            got(whole, xr.at[j])
            remote(half, half, sx, fr.at[j], me, left).start()
            remote(whole, whole, sx, pr.at[j], me, mate).start()

        @pl.when(i >= 2)
        def _():
            j = i - 2
            at = plane_rows(j)
            whole = tok.at[far, pl.ds(at, NY)]
            got(tok.at[far, pl.ds(at, NY // 2)], fl.at[j])
            got(tok.at[far, pl.ds(at + NY // 2, NY // 2)], fr.at[j])
            remote(whole, whole, sx, pf.at[j], me, mate).start()

    def side_of(d, side):
        way = 1 - 2 * side
        return (mz + NZ - way) % NZ * NY + my, (mz + NZ + way * (d - 1)) % NZ

    def build(d):
        def one(side):
            src, z = side_of(d, side)
            s0, s1 = near[side, 0:1, :], near[side, 1:2, :]
            base = 8 + (side * 4 + d - 1) * 8
            if d < 4:
                outbox[pl.ds(base, 8)] = pack_plane(blk[side], s0, s1, z)
            else:
                outbox[pl.ds(base, 4)] = pack_half(blk[side], s0, s1, z, side)
            if d == 1:
                tok[t, src] = outbox[pl.ds(base + my * 2, 2)]

        loop(2, one)

    def relay(d):
        def one(side):
            src, z = side_of(d, side)
            base = 8 + (side * 4 + d - 1) * 8
            group = 7 if d == 4 else 2 * d - 1 + side
            for dy in range(1 if d == 1 else 0, NY):
                y = (my + dy) % NY
                if d < 4:
                    remote(outbox.at[pl.ds(base + y * 2, 2)], tok.at[t, src], st, own.at[group], z * NY + y, t).start()
                else:
                    remote(outbox.at[base + y], tok.at[t, src, side], st, own.at[group], z * NY + y, t).start()

        loop(2, one)

    loop(1, gather)
    for side in range(2):
        got(near.at[side], rnear.at[side])
        got(blk.at[side], rblk.at[side])
    build(2)
    relay(2)
    build(1)
    relay(1)
    build(3)
    relay(3)
    loop(2, gather, 1)
    build(4)
    relay(4)
    loop(3, gather, 2)
    cast_gu(0)
    send_d(0, 5, NZ)
    send_gu(0)
    loop(4, gather, 3)
    cast_gu(1)
    cast_d(1)
    send_gu(1)
    send_d(1)
    loop(NZ + 2, gather, 4)

    def gathered(i):
        at = pl.ds(plane_rows(i), NY)
        got(tok.at[mate, at], po.at[i])
        got(tok.at[left + 1 - 2 * mc, at], pl_.at[i])
        got(tok.at[right + 1 - 2 * mc, at], pr.at[i])
        got(tok.at[far + 1 - 2 * mc, at], pf.at[i])

    loop(NZ, gathered)

    CH = 8
    NCH = NFS // CH
    CR = CH * CAP

    def chunk_of(k):
        step = (2 + ((k + 1) // 2) * (1 - 2 * (k % 2))) % NCH
        return (mz // 2 + step) % NCH

    def expert(e):
        got(wsend_gu.at[e, pl.ds(0, NFS - 1)], rwgu.at[e])

        def hrows(k):
            return pl.ds(pl.multiple_of(chunk_of(k) * CR, CR), CR)

        def send_h(k):
            piece = hid.at[t, e, hrows(k)]
            remote(piece, piece, sh.at[e], hxl.at[e, k], me, right).start()
            remote(piece, piece, sh.at[e], hxr.at[e, k], me, left).start()
            remote(piece, piece, sh.at[e], hpo.at[e, k], me, mate).start()

        def forward_h(k):
            base = pl.multiple_of(chunk_of(k) * CR, CR)
            whole = hid.at[left, e, pl.ds(base, CR)]
            half = hid.at[left, e, pl.ds(base, CR // 2)]
            got(whole, hxl.at[e, k])
            remote(half, half, sh.at[e], hfl.at[e, k], me, right).start()
            remote(whole, whole, sh.at[e], hpl.at[e, k], me, mate).start()
            whole = hid.at[right, e, pl.ds(base, CR)]
            half = hid.at[right, e, pl.ds(base + CR // 2, CR // 2)]
            got(whole, hxr.at[e, k])
            remote(half, half, sh.at[e], hfr.at[e, k], me, left).start()
            remote(whole, whole, sh.at[e], hpr.at[e, k], me, mate).start()

        def pass_h(k):
            base = pl.multiple_of(chunk_of(k) * CR, CR)
            whole = hid.at[far, e, pl.ds(base, CR)]
            got(hid.at[far, e, pl.ds(base, CR // 2)], hfl.at[e, k])
            got(hid.at[far, e, pl.ds(base + CR // 2, CR // 2)], hfr.at[e, k])
            remote(whole, whole, sh.at[e], hpf.at[e, k], me, mate).start()

        def up_step(k):
            @pl.when(k < NCH)
            def _():
                senders = pl.ds(chunk_of(k) * CH, CH)
                acc = jnp.zeros((CR, 256), F32)
                for p in range(NTP):
                    x = tok[p, senders, e].reshape(CR, 256)
                    acc = acc + jnp.dot(x, wgu[e, p * 256 : (p + 1) * 256, :], preferred_element_type=F32)
                gate, up = acc[:, 0:128], acc[:, 128:256]
                hid[t, e, hrows(k), :] = (gate / (1.0 + jnp.exp(-gate)) * up).astype(BF16)

            @pl.when((k >= 1) & (k < NCH + 1))
            def _():
                send_h(k - 1)

            @pl.when((k >= 2) & (k < NCH + 2))
            def _():
                forward_h(k - 2)

            @pl.when(k >= 3)
            def _():
                pass_h(k - 3)

        loop(NCH + 3, up_step)

        got(wsend_d.at[e, pl.ds(0, NFS - 1)], rwd.at[e])

        def send_r(k):
            plane = chunk_of(k) * 2
            for n in range(CH):
                s = (plane + n // NY) * NY + (my + n) % NY

                def go(s=s):
                    remote(eo.at[e, s], ret[e].at[me], sr.at[e], rr.at[e], s, t).start()

                if n % NY == 0:
                    pl.when(s != me)(go)
                else:
                    go()

        def down_step(k):
            @pl.when(k < NCH)
            def _():
                rows = hrows(k)
                got(hid.at[mate, e, rows], hpo.at[e, k])
                got(hid.at[left + 1 - 2 * mc, e, rows], hpl.at[e, k])
                got(hid.at[right + 1 - 2 * mc, e, rows], hpr.at[e, k])
                got(hid.at[far + 1 - 2 * mc, e, rows], hpf.at[e, k])
                acc = jnp.zeros((CR, 256), F32)
                for q in range(NX):
                    h = jnp.concatenate([hid[2 * q, e, rows, :], hid[2 * q + 1, e, rows, :]], axis=1)
                    acc = acc + jnp.dot(h, wd[e, q * 256 : (q + 1) * 256, :], preferred_element_type=F32)
                eo[e, pl.ds(chunk_of(k) * CH, CH)] = acc.astype(BF16).reshape(CH, CAP, 256)

            @pl.when(k >= 1)
            def _():
                send_r(k - 1)

        loop(NCH + 1, down_step)
        ret[e][me] = eo[e, me]

    expert(0)
    expert(1)

    r0, r1 = rt_ref[0:1, :], rt_ref[1:2, :]
    rank0, rank1 = slots[0:1, :] - r0 * CAP, slots[1:2, :] - r1 * CAP
    loads[8].wait()
    a0, a1 = at_ref[0:1, :], at_ref[1:2, :]
    total = a0 + a1

    def keys(r, rank, e):
        key = jnp.right_shift(r, 1) * CAP + rank
        return jnp.where(jnp.bitwise_and(r, 1) == e, key, -1).astype(F32)

    packed = jnp.concatenate(
        [keys(r0, rank0, 0), keys(r1, rank1, 0), keys(r0, rank0, 1), keys(r1, rank1, 1), a0 / total, a1 / total,
         jnp.zeros((122, 768), F32)],
        axis=0,
    )
    macc[...] = jnp.concatenate([packed.T, jnp.zeros((768, 128), F32)], axis=1)

    def weigh(b):
        rows = pl.ds(pl.multiple_of(b * 64, 64), 64)
        columns = macc[rows, 0:128]
        index = lax.broadcasted_iota(jnp.int32, (64, NFS * CAP), 1).astype(F32)
        for e in range(2):
            first = jnp.where(index == columns[:, 2 * e : 2 * e + 1], columns[:, 4:5], 0.0)
            second = jnp.where(index == columns[:, 2 * e + 1 : 2 * e + 2], columns[:, 5:6], 0.0)
            wcomb[e][rows, :] = (first + second).astype(BF16)

    loop(12, weigh)

    got(ret0.at[pl.ds(0, NFS - 1)], rr.at[0])

    def mix_first(b):
        rows = pl.ds(pl.multiple_of(b * 256, 256), 256)
        macc[rows, :] = jnp.dot(wcomb0[rows, :], ret0[...].reshape(NFS * CAP, 256), preferred_element_type=F32)

    loop(3, mix_first)
    got(ret1.at[pl.ds(0, NFS - 1)], rr.at[1])

    for e in range(2):
        sent(wsend_gu.at[e, pl.ds(0, NFS - 1)], swgu.at[e])
        sent(wsend_d.at[e, pl.ds(0, NFS - 1)], swd.at[e])
        sent(hid.at[pl.ds(0, 7), e], sh.at[e])
        sent(eo.at[e, pl.ds(0, NFS - 1)], sr.at[e])
    sent(outbox.at[pl.ds(0, 58)], st)
    sent(blk, sa.at[0])
    sent(near, sa.at[1])
    sent(tok.at[pl.ds(0, 7)], sx)


def finish(wgu, wd, macc, wcomb1, ret1, mixed_out, gate_out, up_out, down_out, mixed, sem):
    copies = [
        pltpu.make_async_copy(wgu.at[:, :, pl.ds(0, 128)], gate_out, sem.at[0]),
        pltpu.make_async_copy(wgu.at[:, :, pl.ds(128, 128)], up_out, sem.at[1]),
        pltpu.make_async_copy(wd, down_out, sem.at[2]),
    ]
    for c in copies:
        c.start()
    for b in range(3):
        rows = pl.ds(b * 256, 256)
        odd = jnp.dot(wcomb1[rows, :], ret1[...].reshape(NFS * CAP, 256), preferred_element_type=F32)
        mixed[rows, :] = (macc[rows, :] + odd).astype(BF16)
    last = pltpu.make_async_copy(mixed, mixed_out, sem.at[3])
    last.start()
    for c in copies + [last]:
        c.wait()


def per_device(prompt, routes, affinity, norm_gain, gate_master, up_master, down_master):
    vmem = pl.BlockSpec(memory_space=pltpu.VMEM)
    hbm = pl.BlockSpec(memory_space=pl.ANY)
    dma = pltpu.SemaphoreType.DMA
    scratch = [
        pltpu.VMEM((2, 768), jnp.int32),
        pltpu.VMEM((2, 768), F32),
        pltpu.VMEM((1, 64), F32),
        pltpu.VMEM((768, 2048), BF16),
        pltpu.VMEM((2, 32, 64, 128), F32),
        pltpu.VMEM((2, 32, 64, 128), F32),
        pltpu.VMEM((2, 32, 32, 256), F32),
        pltpu.VMEM((2, 32, 64, 256), BF16),
        pltpu.VMEM((2, 32, 32, 256), BF16),
        pltpu.VMEM((768, 256), BF16),
        pltpu.VMEM((2, 768, 256), BF16),
        pltpu.VMEM((2, 8, 768), jnp.int32),
        pltpu.VMEM((9 * 8, CAP, 256), BF16),
        pltpu.VMEM((NTP, NFS, 2, CAP, 256), BF16),
        pltpu.VMEM((NTP, 2, NFS * CAP, 128), BF16),
        pltpu.VMEM((2, NFS, CAP, 256), BF16),
        pltpu.VMEM((NFS, CAP, 256), BF16),
        pltpu.VMEM((768, NFS * CAP), BF16),
        pltpu.VMEM((8, 768), jnp.int32),
        dma((10,)),
        dma((2,)), dma((2,)), dma((2,)),
        dma((2,)), dma((2,)), dma((2,)), dma((2,)),
        dma, dma,
        *[dma((NZ,)) for _ in range(9)],
        dma((2,)),
        *[dma((2, 4)) for _ in range(8)],
        dma((2,)), dma((2,)),
    ]
    landed = pl.pallas_call(
        kernel,
        out_shape=(
            pltpu.VMEM((2, 2048, 256), BF16),
            pltpu.VMEM((2, 1024, 256), BF16),
            pltpu.VMEM((768, 256), F32),
            pltpu.VMEM((768, NFS * CAP), BF16),
            pltpu.VMEM((NFS, CAP, 256), BF16),
        ),
        in_specs=[hbm] * 7,
        out_specs=(vmem,) * 5,
        scratch_shapes=scratch,
        compiler_params=pltpu.CompilerParams(
            collective_id=0, has_side_effects=True, vmem_limit_bytes=50 * 1024 * 1024
        ),
        name="hand_off",
    )(
        routes.T,
        affinity.T,
        norm_gain.reshape(1, 64),
        prompt,
        gate_master.reshape(32, 2, 64, 128),
        up_master.reshape(32, 2, 64, 128),
        down_master.reshape(32, 2, 32, 256),
    )
    return pl.pallas_call(
        finish,
        out_shape=(
            jax.ShapeDtypeStruct((768, 256), BF16),
            jax.ShapeDtypeStruct((2, 2048, 128), BF16),
            jax.ShapeDtypeStruct((2, 2048, 128), BF16),
            jax.ShapeDtypeStruct((2, 1024, 256), BF16),
        ),
        in_specs=[vmem] * 5,
        out_specs=(hbm,) * 4,
        scratch_shapes=[pltpu.VMEM((768, 256), BF16), dma((4,))],
        compiler_params=pltpu.CompilerParams(vmem_limit_bytes=8 * 1024 * 1024),
        name="finish",
    )(*landed)


def solution(mesh):
    in_specs = (
        P("fs", None),
        P("fs", None),
        P("fs", None),
        P("fs"),
        P(None, "fs", "tp"),
        P(None, "fs", "tp"),
        P(None, "fs", "tp"),
    )
    out_specs = (P("fs", "tp"), P("fs", None, "tp"), P("fs", None, "tp"), P("fs", None, "tp"))
    return jax.shard_map(
        per_device, mesh=mesh, in_specs=in_specs, out_specs=out_specs, check_vma=False
    )
```

```python
import jax
import jax.numpy as jnp
from jax import lax
from jax.experimental import pallas as pl
from jax.experimental.pallas import tpu as pltpu
from jax.sharding import PartitionSpec as P

MESH = pl.DeviceIdType.MESH
norm_eps = 1e-06

NZ, NY, NX = 8, 4, 4
NFS = NZ * NY
NTP = NX * 2
CAP = 48
BF16, F32 = jnp.bfloat16, jnp.float32


def plane_step(i):
    return NZ + ((i + 1) // 2) * (2 * (i % 2) - 1)


def loop(count, body, start=0):
    def step(i, carry):
        body(i)
        return carry

    lax.fori_loop(start, count, step, 0)


def kernel(
    rt_hbm, at_hbm, gain_hbm, prompt_ref, gate_ref, up_ref, down_ref,
    wgu, wd, macc, wcomb1, ret1,
    rt_ref, at_ref, gain_ref, pbuf, gbuf, ubuf, dbuf, wsend_gu, wsend_d, nm, blk, near, outbox, tok, hid, eo, ret0, wcomb0,
    slots, load_sem, sa, rblk, rnear, swgu, swd, rwgu, rwd, st, sx, own, xl, xr, fl, fr, po, pl_, pr, pf,
    sh, hxl, hxr, hfl, hfr, hpo, hpl, hpr, hpf, sr, rr,
):
    me = lax.axis_index("fs")
    t = lax.axis_index("tp")
    mz, my = me // NY, me % NY
    mx, mc = t // 2, t % 2
    right = ((mx + 1) % NX) * 2 + mc
    left = ((mx + NX - 1) % NX) * 2 + mc
    far = ((mx + 2) % NX) * 2 + mc
    mate = mx * 2 + 1 - mc

    ret, wcomb = (ret0, ret1), (wcomb0, wcomb1)

    def load(n, src, dst):
        return pltpu.make_async_copy(src, dst, load_sem.at[n])

    loads = [
        load(3, down_ref.at[:, 0], dbuf.at[0]),
        load(2, prompt_ref, pbuf),
        load(0, gate_ref.at[:, 0], gbuf.at[0]),
        load(1, up_ref.at[:, 0], ubuf.at[0]),
        load(4, gate_ref.at[:, 1], gbuf.at[1]),
        load(5, up_ref.at[:, 1], ubuf.at[1]),
        load(6, down_ref.at[:, 1], dbuf.at[1]),
        load(7, rt_hbm, rt_ref),
        load(8, at_hbm, at_ref),
        load(9, gain_hbm, gain_ref),
    ]
    for n in (0, 1, 7, 9, 2, 3, 4, 5, 6, 8):
        loads[n].start()

    barrier = pltpu.get_barrier_semaphore()

    def greet(i):
        pl.semaphore_signal(barrier, inc=1, device_id=((me + 1 + i) % NFS, t), device_id_type=MESH)

    loop(NFS - 1, greet)
    for other in (right, left, mate):
        pl.semaphore_signal(barrier, inc=1, device_id=(me, other), device_id_type=MESH)

    def remote(src, dst, ssem, rsem, fs, tp):
        return pltpu.make_async_remote_copy(
            src_ref=src, dst_ref=dst, send_sem=ssem, recv_sem=rsem, device_id=(fs, tp), device_id_type=MESH
        )

    def got(ref, sem):
        remote(ref, ref, sem, sem, me, t).wait_recv()

    def sent(ref, sem):
        remote(ref, ref, sem, sem, me, t).wait_send()

    def to_peers(send, first=0, last=NZ):
        def plane(i):
            z = (mz + plane_step(i)) % NZ
            for dy in range(NY):
                dst = z * NY + (my + dy) % NY
                if dy == 0:
                    @pl.when(i > 0)
                    def _():
                        send(dst)
                else:
                    send(dst)

        loop(last, plane, first)

    def cast_gu(e):
        if e == 0:
            loads[9].wait()
        loads[2 if e == 0 else 4].wait()
        loads[3 if e == 0 else 5].wait()

        diagonal = lax.broadcasted_iota(jnp.int32, (64, 64), 0) == lax.broadcasted_iota(jnp.int32, (64, 64), 1)
        column = jnp.sum(jnp.where(diagonal, gain_ref[...], 0.0), axis=1, keepdims=True)
        gain = jnp.broadcast_to(column, (64, 128))[None]

        def block(b):
            rows = pl.ds(b * 4, 4)
            wsend_gu[e, rows, :, 0:128] = (gbuf[e, rows] * gain).astype(BF16)
            wsend_gu[e, rows, :, 128:256] = (ubuf[e, rows] * gain).astype(BF16)

        loop(8, block)
        wgu[e, pl.ds(pl.multiple_of(me * 64, 64), 64), :] = wsend_gu[e, me]

    def send_gu(e, first=0, last=NZ):
        def send(dst):
            remote(
                wsend_gu.at[e, dst], wgu.at[e, pl.ds(pl.multiple_of(me * 64, 64), 64)], swgu.at[e], rwgu.at[e], dst, t
            ).start()

        to_peers(send, first, last)

    def cast_d(e):
        loads[0 if e == 0 else 6].wait()

        def block(b):
            rows = pl.ds(b * 4, 4)
            wsend_d[e, rows] = dbuf[e, rows].astype(BF16)

        loop(8, block)
        wd[e, pl.ds(pl.multiple_of(me * 32, 32), 32), :] = wsend_d[e, me]

    def send_d(e, first=0, last=NZ):
        def send(dst):
            remote(
                wsend_d.at[e, dst], wd.at[e, pl.ds(pl.multiple_of(me * 32, 32), 32)], swd.at[e], rwd.at[e], dst, t
            ).start()

        to_peers(send, first, last)

    cast_d(0)
    pl.semaphore_wait(barrier, NFS - 1 + 3)
    send_d(0, 0, 5)

    loads[1].wait()

    def norm(b):
        rows = pl.ds(pl.multiple_of(b * 64, 64), 64)
        x = pbuf[rows, :].astype(F32)
        scale = lax.rsqrt(jnp.mean(x * x, axis=-1, keepdims=True) + norm_eps)
        mine = pbuf[rows, pl.ds(pl.multiple_of(t * 256, 256), 256)].astype(F32)
        nm[rows, :] = (mine * scale).astype(BF16)

    loop(12, norm)
    above, below = (mz + 1) % NZ * NY + my, (mz + NZ - 1) % NZ * NY + my
    remote(nm, blk.at[0], sa.at[0], rblk.at[0], above, t).start()
    remote(nm, blk.at[1], sa.at[0], rblk.at[1], below, t).start()

    loads[7].wait()
    r0, r1 = rt_ref[0:1, :], rt_ref[1:2, :]
    experts = lax.broadcasted_iota(jnp.int32, (64, 768), 0)
    oh0 = (experts == r0).astype(F32)
    oh1 = (experts == r1).astype(F32)
    before = lax.broadcasted_iota(jnp.int32, (768, 768), 0) < lax.broadcasted_iota(jnp.int32, (768, 768), 1)
    count = jnp.dot((oh0 + oh1).astype(BF16), before.astype(F32).astype(BF16), preferred_element_type=F32)
    rank0 = jnp.sum(count * oh0, axis=0, keepdims=True).astype(jnp.int32)
    rank1 = jnp.sum(count * oh1, axis=0, keepdims=True).astype(jnp.int32)
    slots[...] = jnp.concatenate([r0 * CAP + rank0, r1 * CAP + rank1], axis=0)

    def pack(block, s0, s1, index):
        hit = (index == s0) | (index == s1)
        rows = jnp.dot(hit.astype(F32).astype(BF16), block, preferred_element_type=F32)
        return rows.astype(BF16)

    def pack_plane(block, s0, s1, z):
        index = lax.broadcasted_iota(jnp.int32, (8 * CAP, 768), 0) + z * (8 * CAP)
        return pack(block, s0, s1, index).reshape(8, CAP, 256)

    def pack_half(block, s0, s1, z, e):
        turn = lax.broadcasted_iota(jnp.int32, (4, CAP, 768), 0) * (2 * CAP)
        index = turn + lax.broadcasted_iota(jnp.int32, (4, CAP, 768), 1) + (z * (8 * CAP) + e * CAP)
        return pack(block, s0, s1, index.reshape(4 * CAP, 768)).reshape(4, CAP, 256)

    outbox[0:8] = pack_plane(nm[...], slots[0:1, :], slots[1:2, :], mz)
    remote(slots, near.at[0], sa.at[1], rnear.at[0], above, t).start()
    remote(slots, near.at[1], sa.at[1], rnear.at[1], below, t).start()
    remote(slots, near.at[2], sa.at[1], rnear.at[2], (mz + 2) % NZ * NY + my, t).start()
    remote(slots, near.at[3], sa.at[1], rnear.at[3], (mz + NZ - 2) % NZ * NY + my, t).start()
    tok[t, me] = outbox[pl.ds(my * 2, 2)]
    for dy in range(1, NY):
        y = (my + dy) % NY
        remote(outbox.at[pl.ds(y * 2, 2)], tok.at[t, me], st, own.at[0], mz * NY + y, t).start()
    send_d(0, 5, 7)

    def plane_rows(i):
        z = (mz + 2 * NZ - plane_step(i)) % NZ
        return z * NY

    def gather(i):
        @pl.when(i < NZ)
        def _():
            at = plane_rows(i)

            @pl.when(i > 4)
            def _():
                got(tok.at[t, pl.ds(at, NY)], own.at[i])

            @pl.when(i <= 4)
            def _():
                got(tok.at[t, pl.ds(at, NY - 1)], own.at[i])

            piece = tok.at[t, pl.ds(at, NY)]
            remote(piece, piece, sx, xl.at[i], me, right).start()
            remote(piece, piece, sx, xr.at[i], me, left).start()
            remote(piece, piece, sx, po.at[i], me, mate).start()

        @pl.when((i >= 1) & (i < NZ + 1))
        def _():
            j = i - 1
            at = plane_rows(j)
            whole = tok.at[left, pl.ds(at, NY)]
            half = tok.at[left, pl.ds(at, NY // 2)]
            got(whole, xl.at[j])
            remote(half, half, sx, fl.at[j], me, right).start()
            remote(whole, whole, sx, pl_.at[j], me, mate).start()
            whole = tok.at[right, pl.ds(at, NY)]
            half = tok.at[right, pl.ds(at + NY // 2, NY // 2)]
            got(whole, xr.at[j])
            remote(half, half, sx, fr.at[j], me, left).start()
            remote(whole, whole, sx, pr.at[j], me, mate).start()

        @pl.when(i >= 2)
        def _():
            j = i - 2
            at = plane_rows(j)
            whole = tok.at[far, pl.ds(at, NY)]
            got(tok.at[far, pl.ds(at, NY // 2)], fl.at[j])
            got(tok.at[far, pl.ds(at + NY // 2, NY // 2)], fr.at[j])
            remote(whole, whole, sx, pf.at[j], me, mate).start()

    def side_of(d, side):
        way = 1 - 2 * side
        dist = min(d, 2)
        held = side + 2 * (dist - 1)
        return held, (mz + NZ - way * dist) % NZ * NY + my, (mz + NZ + way * (d - dist)) % NZ

    def build(d):
        def one(side):
            held, src, z = side_of(d, side)
            s0, s1 = near[held, 0:1, :], near[held, 1:2, :]
            base = 8 + (side * 4 + d - 1) * 8
            if d < 4:
                outbox[pl.ds(base, 8)] = pack_plane(blk[held], s0, s1, z)
            else:
                outbox[pl.ds(base, 4)] = pack_half(blk[held], s0, s1, z, side)
            if d <= 2:
                tok[t, src] = outbox[pl.ds(base + my * 2, 2)]

        loop(2, one)

    def relay(d):
        def one(side):
            held, src, z = side_of(d, side)
            base = 8 + (side * 4 + d - 1) * 8
            group = 7 if d == 4 else 2 * d - 1 + side
            for dy in range(1 if d <= 2 else 0, NY):
                y = (my + dy) % NY
                if d < 4:
                    remote(outbox.at[pl.ds(base + y * 2, 2)], tok.at[t, src], st, own.at[group], z * NY + y, t).start()
                else:
                    remote(outbox.at[base + y], tok.at[t, src, side], st, own.at[group], z * NY + y, t).start()

        loop(2, one)

    loop(1, gather)
    for side in range(2):
        got(near.at[side], rnear.at[side])
        got(blk.at[side], rblk.at[side])
        remote(blk.at[side], blk.at[2 + side], sa.at[0], rblk.at[2 + side], below if side else above, t).start()
    build(1)
    relay(1)
    send_d(0, 7, NZ)
    cast_gu(0)
    send_gu(0, 0, 5)
    loop(2, gather, 1)
    for side in range(2, 4):
        got(near.at[side], rnear.at[side])
        got(blk.at[side], rblk.at[side])
    build(2)
    relay(2)
    build(3)
    relay(3)
    loop(3, gather, 2)
    build(4)
    relay(4)
    send_gu(0, 5, NZ)
    cast_gu(1)
    send_gu(1)
    loop(4, gather, 3)
    cast_d(1)
    send_d(1)
    loop(NZ, gather, 4)

    def gathered(i):
        at = pl.ds(plane_rows(i), NY)
        got(tok.at[mate, at], po.at[i])
        got(tok.at[left + 1 - 2 * mc, at], pl_.at[i])
        got(tok.at[right + 1 - 2 * mc, at], pr.at[i])
        got(tok.at[far + 1 - 2 * mc, at], pf.at[i])


    CH = 8
    NCH = NFS // CH
    CR = CH * CAP

    def chunk_of(k, e):
        if e == 0:
            step = ((k + 1) % 3 + 1) * ((k + 3) // 4)
        else:
            step = 2 + ((k + 1) // 2) * (1 - 2 * (k % 2))
        return (mz // 2 + step) % NCH

    def phases(e):

        def hrows(k):
            return pl.ds(pl.multiple_of(chunk_of(k, e) * CR, CR), CR)

        def send_h(k):
            piece = hid.at[t, e, hrows(k)]
            remote(piece, piece, sh.at[e], hxl.at[e, k], me, right).start()
            remote(piece, piece, sh.at[e], hxr.at[e, k], me, left).start()
            remote(piece, piece, sh.at[e], hpo.at[e, k], me, mate).start()

        def forward_h(k):
            base = pl.multiple_of(chunk_of(k, e) * CR, CR)
            whole = hid.at[left, e, pl.ds(base, CR)]
            half = hid.at[left, e, pl.ds(base, CR // 2)]
            got(whole, hxl.at[e, k])
            remote(half, half, sh.at[e], hfl.at[e, k], me, right).start()
            remote(whole, whole, sh.at[e], hpl.at[e, k], me, mate).start()
            whole = hid.at[right, e, pl.ds(base, CR)]
            half = hid.at[right, e, pl.ds(base + CR // 2, CR // 2)]
            got(whole, hxr.at[e, k])
            remote(half, half, sh.at[e], hfr.at[e, k], me, left).start()
            remote(whole, whole, sh.at[e], hpr.at[e, k], me, mate).start()

        def pass_h(k):
            base = pl.multiple_of(chunk_of(k, e) * CR, CR)
            whole = hid.at[far, e, pl.ds(base, CR)]
            got(hid.at[far, e, pl.ds(base, CR // 2)], hfl.at[e, k])
            got(hid.at[far, e, pl.ds(base + CR // 2, CR // 2)], hfr.at[e, k])
            remote(whole, whole, sh.at[e], hpf.at[e, k], me, mate).start()

        def compute_h(k):
            senders = pl.ds(chunk_of(k, e) * CH, CH)
            acc = jnp.zeros((CR, 256), F32)
            for p in range(NTP):
                x = tok[p, senders, e].reshape(CR, 256)
                acc = acc + jnp.dot(x, wgu[e, p * 256 : (p + 1) * 256, :], preferred_element_type=F32)
            gate, up = acc[:, 0:128], acc[:, 128:256]
            hid[t, e, hrows(k), :] = (gate / (1.0 + jnp.exp(-gate)) * up).astype(BF16)

        def hidden(first, last):
            def step(k):
                pl.when(k < NCH)(lambda: compute_h(k))
                pl.when(k >= 1)(lambda: send_h(k - 1))

            loop(last, step, first)

        def forwarding():
            def step(k):
                pl.when(k < NCH)(lambda: forward_h(k))
                pl.when(k >= 1)(lambda: pass_h(k - 1))

            loop(NCH + 1, step)

        def send_r(k):
            plane = chunk_of(k, e) * 2
            for n in range(CH):
                s = (plane + n // NY) * NY + (my + n) % NY

                def go(s=s):
                    remote(eo.at[e, s], ret[e].at[me], sr.at[e], rr.at[e], s, t).start()

                if n % NY == 0:
                    pl.when(s != me)(go)
                else:
                    go()

        def down_step(k):
            @pl.when(k < NCH)
            def _():
                rows = hrows(k)
                got(hid.at[mate, e, rows], hpo.at[e, k])
                got(hid.at[left + 1 - 2 * mc, e, rows], hpl.at[e, k])
                got(hid.at[right + 1 - 2 * mc, e, rows], hpr.at[e, k])
                got(hid.at[far + 1 - 2 * mc, e, rows], hpf.at[e, k])
                acc = jnp.zeros((CR, 256), F32)
                for q in range(NX):
                    h = jnp.concatenate([hid[2 * q, e, rows, :], hid[2 * q + 1, e, rows, :]], axis=1)
                    acc = acc + jnp.dot(h, wd[e, q * 256 : (q + 1) * 256, :], preferred_element_type=F32)
                eo[e, pl.ds(chunk_of(k, e) * CH, CH)] = acc.astype(BF16).reshape(CH, CAP, 256)

            @pl.when(k >= 1)
            def _():
                send_r(k - 1)

        def returns():
            got(wsend_d.at[e, pl.ds(0, NFS - 1)], rwd.at[e])
            loop(NCH + 1, down_step)
            ret[e][me] = eo[e, me]

        return hidden, forwarding, returns

    hidden_even, forwarding_even, returns_even = phases(0)
    hidden_odd, forwarding_odd, returns_odd = phases(1)
    loop(NZ + 1, gather, NZ)
    loop(3, gathered)
    got(wsend_gu.at[0, pl.ds(0, NFS - 1)], rwgu.at[0])
    hidden_even(0, 1)
    loop(NZ + 2, gather, NZ + 1)
    loop(6, gathered, 3)
    hidden_even(1, 2)
    loop(7, gathered, 6)
    hidden_even(2, 3)
    loop(NZ, gathered, 7)
    hidden_even(3, NCH + 1)
    forwarding_even()
    got(wsend_gu.at[1, pl.ds(0, NFS - 1)], rwgu.at[1])
    hidden_odd(0, NCH + 1)
    returns_even()
    forwarding_odd()
    returns_odd()

    r0, r1 = rt_ref[0:1, :], rt_ref[1:2, :]
    rank0, rank1 = slots[0:1, :] - r0 * CAP, slots[1:2, :] - r1 * CAP
    loads[8].wait()
    a0, a1 = at_ref[0:1, :], at_ref[1:2, :]
    total = a0 + a1

    def keys(r, rank, e):
        key = jnp.right_shift(r, 1) * CAP + rank
        return jnp.where(jnp.bitwise_and(r, 1) == e, key, -1).astype(F32)

    packed = jnp.concatenate(
        [keys(r0, rank0, 0), keys(r1, rank1, 0), keys(r0, rank0, 1), keys(r1, rank1, 1), a0 / total, a1 / total,
         jnp.zeros((122, 768), F32)],
        axis=0,
    )
    macc[...] = jnp.concatenate([packed.T, jnp.zeros((768, 128), F32)], axis=1)

    def weigh(b):
        rows = pl.ds(pl.multiple_of(b * 64, 64), 64)
        columns = macc[rows, 0:128]
        index = lax.broadcasted_iota(jnp.int32, (64, NFS * CAP), 1).astype(F32)
        for e in range(2):
            first = jnp.where(index == columns[:, 2 * e : 2 * e + 1], columns[:, 4:5], 0.0)
            second = jnp.where(index == columns[:, 2 * e + 1 : 2 * e + 2], columns[:, 5:6], 0.0)
            wcomb[e][rows, :] = (first + second).astype(BF16)

    loop(12, weigh)

    got(ret0.at[pl.ds(0, NFS - 1)], rr.at[0])

    def mix_first(b):
        rows = pl.ds(pl.multiple_of(b * 256, 256), 256)
        macc[rows, :] = jnp.dot(wcomb0[rows, :], ret0[...].reshape(NFS * CAP, 256), preferred_element_type=F32)

    loop(3, mix_first)
    got(ret1.at[pl.ds(0, NFS - 1)], rr.at[1])

    for e in range(2):
        sent(wsend_gu.at[e, pl.ds(0, NFS - 1)], swgu.at[e])
        sent(wsend_d.at[e, pl.ds(0, NFS - 1)], swd.at[e])
        sent(hid.at[pl.ds(0, 7), e], sh.at[e])
        sent(eo.at[e, pl.ds(0, NFS - 1)], sr.at[e])
    sent(outbox.at[pl.ds(0, 54)], st)
    sent(blk, sa.at[0])
    sent(near, sa.at[1])
    sent(tok.at[pl.ds(0, 7)], sx)


def finish(wgu, wd, macc, wcomb1, ret1, mixed_out, gate_out, up_out, down_out, mixed, sem):
    copies = [
        pltpu.make_async_copy(wgu.at[:, :, pl.ds(0, 128)], gate_out, sem.at[0]),
        pltpu.make_async_copy(wgu.at[:, :, pl.ds(128, 128)], up_out, sem.at[1]),
        pltpu.make_async_copy(wd, down_out, sem.at[2]),
    ]
    for c in copies:
        c.start()
    for b in range(3):
        rows = pl.ds(b * 256, 256)
        odd = jnp.dot(wcomb1[rows, :], ret1[...].reshape(NFS * CAP, 256), preferred_element_type=F32)
        mixed[rows, :] = (macc[rows, :] + odd).astype(BF16)
    last = pltpu.make_async_copy(mixed, mixed_out, sem.at[3])
    last.start()
    for c in copies + [last]:
        c.wait()


def per_device(prompt, routes, affinity, norm_gain, gate_master, up_master, down_master):
    vmem = pl.BlockSpec(memory_space=pltpu.VMEM)
    hbm = pl.BlockSpec(memory_space=pl.ANY)
    dma = pltpu.SemaphoreType.DMA
    scratch = [
        pltpu.VMEM((2, 768), jnp.int32),
        pltpu.VMEM((2, 768), F32),
        pltpu.VMEM((1, 64), F32),
        pltpu.VMEM((768, 2048), BF16),
        pltpu.VMEM((2, 32, 64, 128), F32),
        pltpu.VMEM((2, 32, 64, 128), F32),
        pltpu.VMEM((2, 32, 32, 256), F32),
        pltpu.VMEM((2, 32, 64, 256), BF16),
        pltpu.VMEM((2, 32, 32, 256), BF16),
        pltpu.VMEM((768, 256), BF16),
        pltpu.VMEM((4, 768, 256), BF16),
        pltpu.VMEM((4, 2, 768), jnp.int32),
        pltpu.VMEM((9 * 8, CAP, 256), BF16),
        pltpu.VMEM((NTP, NFS, 2, CAP, 256), BF16),
        pltpu.VMEM((NTP, 2, NFS * CAP, 128), BF16),
        pltpu.VMEM((2, NFS, CAP, 256), BF16),
        pltpu.VMEM((NFS, CAP, 256), BF16),
        pltpu.VMEM((768, NFS * CAP), BF16),
        pltpu.VMEM((2, 768), jnp.int32),
        dma((10,)),
        dma((2,)), dma((4,)), dma((4,)),
        dma((2,)), dma((2,)), dma((2,)), dma((2,)),
        dma, dma,
        *[dma((NZ,)) for _ in range(9)],
        dma((2,)),
        *[dma((2, 4)) for _ in range(8)],
        dma((2,)), dma((2,)),
    ]
    landed = pl.pallas_call(
        kernel,
        out_shape=(
            pltpu.VMEM((2, 2048, 256), BF16),
            pltpu.VMEM((2, 1024, 256), BF16),
            pltpu.VMEM((768, 256), F32),
            pltpu.VMEM((768, NFS * CAP), BF16),
            pltpu.VMEM((NFS, CAP, 256), BF16),
        ),
        in_specs=[hbm] * 7,
        out_specs=(vmem,) * 5,
        scratch_shapes=scratch,
        compiler_params=pltpu.CompilerParams(
            collective_id=0, has_side_effects=True, vmem_limit_bytes=50 * 1024 * 1024
        ),
        name="hand_off",
    )(
        routes.T,
        affinity.T,
        norm_gain.reshape(1, 64),
        prompt,
        gate_master.reshape(32, 2, 64, 128),
        up_master.reshape(32, 2, 64, 128),
        down_master.reshape(32, 2, 32, 256),
    )
    return pl.pallas_call(
        finish,
        out_shape=(
            jax.ShapeDtypeStruct((768, 256), BF16),
            jax.ShapeDtypeStruct((2, 2048, 128), BF16),
            jax.ShapeDtypeStruct((2, 2048, 128), BF16),
            jax.ShapeDtypeStruct((2, 1024, 256), BF16),
        ),
        in_specs=[vmem] * 5,
        out_specs=(hbm,) * 4,
        scratch_shapes=[pltpu.VMEM((768, 256), BF16), dma((4,))],
        compiler_params=pltpu.CompilerParams(vmem_limit_bytes=8 * 1024 * 1024),
        name="finish",
    )(*landed)


def solution(mesh):
    in_specs = (
        P("fs", None),
        P("fs", None),
        P("fs", None),
        P("fs"),
        P(None, "fs", "tp"),
        P(None, "fs", "tp"),
        P(None, "fs", "tp"),
    )
    out_specs = (P("fs", "tp"), P("fs", None, "tp"), P("fs", None, "tp"), P("fs", None, "tp"))
    return jax.shard_map(
        per_device, mesh=mesh, in_specs=in_specs, out_specs=out_specs, check_vma=False
    )
```

```python
import jax
import jax.numpy as jnp
from jax import lax
from jax.experimental import pallas as pl
from jax.experimental.pallas import tpu as pltpu
from jax.sharding import PartitionSpec as P

MESH = pl.DeviceIdType.MESH
norm_eps = 1e-06

NZ, NY, NX = 8, 4, 4
NFS = NZ * NY
NTP = NX * 2
CAP = 48
BF16, F32 = jnp.bfloat16, jnp.float32


def plane_step(i):
    return NZ + ((i + 1) // 2) * (2 * (i % 2) - 1)


def loop(count, body, start=0):
    def step(i, carry):
        body(i)
        return carry

    lax.fori_loop(start, count, step, 0)


def kernel(
    rt_hbm, at_hbm, gain_hbm, prompt_ref, gate_ref, up_ref, down_ref,
    wgu, wd, macc, wcomb1, ret1,
    rt_ref, at_ref, gain_ref, pbuf, gbuf, ubuf, dbuf, wsend_gu, wsend_d, nm, blk, near, outbox, tok, hid, eo, ret0, wcomb0,
    slots, load_sem, sa, rblk, rnear, swgu, swd, rwgu, rwd, st, sx, own, xl, xr, fl, fr, po, pl_, pr, pf,
    sh, hxl, hxr, hfl, hfr, hpo, hpl, hpr, hpf, sr, rr,
):
    me = lax.axis_index("fs")
    t = lax.axis_index("tp")
    mz, my = me // NY, me % NY
    mx, mc = t // 2, t % 2
    right = ((mx + 1) % NX) * 2 + mc
    left = ((mx + NX - 1) % NX) * 2 + mc
    far = ((mx + 2) % NX) * 2 + mc
    mate = mx * 2 + 1 - mc

    ret, wcomb = (ret0, ret1), (wcomb0, wcomb1)

    def load(n, src, dst):
        return pltpu.make_async_copy(src, dst, load_sem.at[n])

    loads = [
        load(3, down_ref.at[:, 0], dbuf.at[0]),
        load(2, prompt_ref, pbuf),
        load(0, gate_ref.at[:, 0], gbuf.at[0]),
        load(1, up_ref.at[:, 0], ubuf.at[0]),
        load(4, gate_ref.at[:, 1], gbuf.at[1]),
        load(5, up_ref.at[:, 1], ubuf.at[1]),
        load(6, down_ref.at[:, 1], dbuf.at[1]),
        load(7, rt_hbm, rt_ref),
        load(8, at_hbm, at_ref),
        load(9, gain_hbm, gain_ref),
    ]
    for n in (0, 1, 7, 9, 2, 3, 4, 5, 6, 8):
        loads[n].start()

    barrier = pltpu.get_barrier_semaphore()

    def greet(i):
        pl.semaphore_signal(barrier, inc=1, device_id=((me + 1 + i) % NFS, t), device_id_type=MESH)

    loop(NFS - 1, greet)
    for other in (right, left, mate):
        pl.semaphore_signal(barrier, inc=1, device_id=(me, other), device_id_type=MESH)

    def remote(src, dst, ssem, rsem, fs, tp):
        return pltpu.make_async_remote_copy(
            src_ref=src, dst_ref=dst, send_sem=ssem, recv_sem=rsem, device_id=(fs, tp), device_id_type=MESH
        )

    def got(ref, sem):
        remote(ref, ref, sem, sem, me, t).wait_recv()

    def sent(ref, sem):
        remote(ref, ref, sem, sem, me, t).wait_send()

    def to_peers(send, first=0, last=NZ):
        def plane(i):
            z = (mz + plane_step(i)) % NZ
            for dy in range(NY):
                dst = z * NY + (my + dy) % NY
                if dy == 0:
                    @pl.when(i > 0)
                    def _():
                        send(dst)
                else:
                    send(dst)

        loop(last, plane, first)

    def cast_gu(e):
        if e == 0:
            loads[9].wait()
        loads[2 if e == 0 else 4].wait()
        loads[3 if e == 0 else 5].wait()

        diagonal = lax.broadcasted_iota(jnp.int32, (64, 64), 0) == lax.broadcasted_iota(jnp.int32, (64, 64), 1)
        column = jnp.sum(jnp.where(diagonal, gain_ref[...], 0.0), axis=1, keepdims=True)
        gain = jnp.broadcast_to(column, (64, 128))[None]

        def block(b):
            rows = pl.ds(b * 4, 4)
            wsend_gu[e, rows, :, 0:128] = (gbuf[e, rows] * gain).astype(BF16)
            wsend_gu[e, rows, :, 128:256] = (ubuf[e, rows] * gain).astype(BF16)

        loop(8, block)
        wgu[e, pl.ds(pl.multiple_of(me * 64, 64), 64), :] = wsend_gu[e, me]

    def send_gu(e, first=0, last=NZ):
        def send(dst):
            remote(
                wsend_gu.at[e, dst], wgu.at[e, pl.ds(pl.multiple_of(me * 64, 64), 64)], swgu.at[e], rwgu.at[e], dst, t
            ).start()

        to_peers(send, first, last)

    def cast_d(e):
        loads[0 if e == 0 else 6].wait()

        def block(b):
            rows = pl.ds(b * 4, 4)
            wsend_d[e, rows] = dbuf[e, rows].astype(BF16)

        loop(8, block)
        wd[e, pl.ds(pl.multiple_of(me * 32, 32), 32), :] = wsend_d[e, me]

    def send_d(e, first=0, last=NZ):
        def send(dst):
            remote(
                wsend_d.at[e, dst], wd.at[e, pl.ds(pl.multiple_of(me * 32, 32), 32)], swd.at[e], rwd.at[e], dst, t
            ).start()

        to_peers(send, first, last)

    cast_d(0)
    pl.semaphore_wait(barrier, NFS - 1 + 3)
    send_d(0, 0, 3)

    loads[1].wait()

    def norm(b):
        rows = pl.ds(pl.multiple_of(b * 64, 64), 64)
        x = pbuf[rows, :].astype(F32)
        scale = lax.rsqrt(jnp.mean(x * x, axis=-1, keepdims=True) + norm_eps)
        mine = pbuf[rows, pl.ds(pl.multiple_of(t * 256, 256), 256)].astype(F32)
        nm[rows, :] = (mine * scale).astype(BF16)

    loop(12, norm)
    above, below = (mz + 1) % NZ * NY + my, (mz + NZ - 1) % NZ * NY + my
    remote(nm, blk.at[0], sa.at[0], rblk.at[0], above, t).start()
    remote(nm, blk.at[1], sa.at[0], rblk.at[1], below, t).start()

    loads[7].wait()
    r0, r1 = rt_ref[0:1, :], rt_ref[1:2, :]
    experts = lax.broadcasted_iota(jnp.int32, (64, 768), 0)
    oh0 = (experts == r0).astype(F32)
    oh1 = (experts == r1).astype(F32)
    before = lax.broadcasted_iota(jnp.int32, (768, 768), 0) < lax.broadcasted_iota(jnp.int32, (768, 768), 1)
    count = jnp.dot((oh0 + oh1).astype(BF16), before.astype(F32).astype(BF16), preferred_element_type=F32)
    rank0 = jnp.sum(count * oh0, axis=0, keepdims=True).astype(jnp.int32)
    rank1 = jnp.sum(count * oh1, axis=0, keepdims=True).astype(jnp.int32)
    slots[...] = jnp.concatenate([r0 * CAP + rank0, r1 * CAP + rank1], axis=0)

    def pack(block, s0, s1, index):
        hit = (index == s0) | (index == s1)
        rows = jnp.dot(hit.astype(F32).astype(BF16), block, preferred_element_type=F32)
        return rows.astype(BF16)

    def pack_plane(block, s0, s1, z):
        index = lax.broadcasted_iota(jnp.int32, (8 * CAP, 768), 0) + z * (8 * CAP)
        return pack(block, s0, s1, index).reshape(8, CAP, 256)

    def pack_half(block, s0, s1, z, e):
        turn = lax.broadcasted_iota(jnp.int32, (4, CAP, 768), 0) * (2 * CAP)
        index = turn + lax.broadcasted_iota(jnp.int32, (4, CAP, 768), 1) + (z * (8 * CAP) + e * CAP)
        return pack(block, s0, s1, index.reshape(4 * CAP, 768)).reshape(4, CAP, 256)

    outbox[0:8] = pack_plane(nm[...], slots[0:1, :], slots[1:2, :], mz)
    remote(slots, near.at[0], sa.at[1], rnear.at[0], above, t).start()
    remote(slots, near.at[1], sa.at[1], rnear.at[1], below, t).start()
    remote(slots, near.at[2], sa.at[1], rnear.at[2], (mz + 2) % NZ * NY + my, t).start()
    remote(slots, near.at[3], sa.at[1], rnear.at[3], (mz + NZ - 2) % NZ * NY + my, t).start()
    tok[t, me] = outbox[pl.ds(my * 2, 2)]
    for dy in range(1, NY):
        y = (my + dy) % NY
        remote(outbox.at[pl.ds(y * 2, 2)], tok.at[t, me], st, own.at[0], mz * NY + y, t).start()
    send_d(0, 3, 5)

    def plane_rows(i):
        z = (mz + 2 * NZ - plane_step(i)) % NZ
        return z * NY

    def gather(i):
        @pl.when(i < NZ)
        def _():
            at = plane_rows(i)

            @pl.when(i > 4)
            def _():
                got(tok.at[t, pl.ds(at, NY)], own.at[i])

            @pl.when(i <= 4)
            def _():
                got(tok.at[t, pl.ds(at, NY - 1)], own.at[i])

            piece = tok.at[t, pl.ds(at, NY)]
            remote(piece, piece, sx, xl.at[i], me, right).start()
            remote(piece, piece, sx, xr.at[i], me, left).start()
            remote(piece, piece, sx, po.at[i], me, mate).start()

        @pl.when((i >= 1) & (i < NZ + 1))
        def _():
            j = i - 1
            at = plane_rows(j)
            whole = tok.at[left, pl.ds(at, NY)]
            half = tok.at[left, pl.ds(at, NY // 2)]
            got(whole, xl.at[j])
            remote(half, half, sx, fl.at[j], me, right).start()
            remote(whole, whole, sx, pl_.at[j], me, mate).start()
            whole = tok.at[right, pl.ds(at, NY)]
            half = tok.at[right, pl.ds(at + NY // 2, NY // 2)]
            got(whole, xr.at[j])
            remote(half, half, sx, fr.at[j], me, left).start()
            remote(whole, whole, sx, pr.at[j], me, mate).start()

        @pl.when(i >= 2)
        def _():
            j = i - 2
            at = plane_rows(j)
            whole = tok.at[far, pl.ds(at, NY)]
            got(tok.at[far, pl.ds(at, NY // 2)], fl.at[j])
            got(tok.at[far, pl.ds(at + NY // 2, NY // 2)], fr.at[j])
            remote(whole, whole, sx, pf.at[j], me, mate).start()

    def side_of(d, side):
        way = 1 - 2 * side
        dist = min(d, 2)
        held = side + 2 * (dist - 1)
        return held, (mz + NZ - way * dist) % NZ * NY + my, (mz + NZ + way * (d - dist)) % NZ

    def build(d):
        def one(side):
            held, src, z = side_of(d, side)
            s0, s1 = near[held, 0:1, :], near[held, 1:2, :]
            base = 8 + (side * 4 + d - 1) * 8
            if d < 4:
                outbox[pl.ds(base, 8)] = pack_plane(blk[held], s0, s1, z)
            else:
                outbox[pl.ds(base, 4)] = pack_half(blk[held], s0, s1, z, side)
            if d <= 2:
                tok[t, src] = outbox[pl.ds(base + my * 2, 2)]

        loop(2, one)

    def relay(d):
        def one(side):
            held, src, z = side_of(d, side)
            base = 8 + (side * 4 + d - 1) * 8
            group = 7 if d == 4 else 2 * d - 1 + side
            for dy in range(1 if d <= 2 else 0, NY):
                y = (my + dy) % NY
                if d < 4:
                    remote(outbox.at[pl.ds(base + y * 2, 2)], tok.at[t, src], st, own.at[group], z * NY + y, t).start()
                else:
                    remote(outbox.at[base + y], tok.at[t, src, side], st, own.at[group], z * NY + y, t).start()

        loop(2, one)

    loop(1, gather)
    for side in range(2):
        got(near.at[side], rnear.at[side])
        got(blk.at[side], rblk.at[side])
        remote(blk.at[side], blk.at[2 + side], sa.at[0], rblk.at[2 + side], below if side else above, t).start()
    build(1)
    relay(1)
    send_d(0, 5, NZ)
    cast_gu(0)
    send_gu(0, 0, 3)
    loop(2, gather, 1)
    for side in range(2, 4):
        got(near.at[side], rnear.at[side])
        got(blk.at[side], rblk.at[side])
    build(2)
    relay(2)
    build(3)
    relay(3)
    loop(3, gather, 2)
    build(4)
    relay(4)
    send_gu(0, 3, NZ)
    cast_gu(1)
    send_gu(1)
    loop(4, gather, 3)
    cast_d(1)
    send_d(1)
    loop(NZ, gather, 4)

    def gathered(i):
        at = pl.ds(plane_rows(i), NY)
        got(tok.at[mate, at], po.at[i])
        got(tok.at[left + 1 - 2 * mc, at], pl_.at[i])
        got(tok.at[right + 1 - 2 * mc, at], pr.at[i])
        got(tok.at[far + 1 - 2 * mc, at], pf.at[i])


    CH = 8
    NCH = NFS // CH
    CR = CH * CAP

    def chunk_of(k, e):
        if e == 0:
            step = ((k + 1) % 3 + 1) * ((k + 3) // 4)
        else:
            step = 2 + ((k + 1) // 2) * (1 - 2 * (k % 2))
        return (mz // 2 + step) % NCH

    def phases(e):

        def hrows(k):
            return pl.ds(pl.multiple_of(chunk_of(k, e) * CR, CR), CR)

        def send_h(k):
            piece = hid.at[t, e, hrows(k)]
            remote(piece, piece, sh.at[e], hxl.at[e, k], me, right).start()
            remote(piece, piece, sh.at[e], hxr.at[e, k], me, left).start()
            remote(piece, piece, sh.at[e], hpo.at[e, k], me, mate).start()

        def forward_h(k):
            base = pl.multiple_of(chunk_of(k, e) * CR, CR)
            whole = hid.at[left, e, pl.ds(base, CR)]
            half = hid.at[left, e, pl.ds(base, CR // 2)]
            got(whole, hxl.at[e, k])
            remote(half, half, sh.at[e], hfl.at[e, k], me, right).start()
            remote(whole, whole, sh.at[e], hpl.at[e, k], me, mate).start()
            whole = hid.at[right, e, pl.ds(base, CR)]
            half = hid.at[right, e, pl.ds(base + CR // 2, CR // 2)]
            got(whole, hxr.at[e, k])
            remote(half, half, sh.at[e], hfr.at[e, k], me, left).start()
            remote(whole, whole, sh.at[e], hpr.at[e, k], me, mate).start()

        def pass_h(k):
            base = pl.multiple_of(chunk_of(k, e) * CR, CR)
            whole = hid.at[far, e, pl.ds(base, CR)]
            got(hid.at[far, e, pl.ds(base, CR // 2)], hfl.at[e, k])
            got(hid.at[far, e, pl.ds(base + CR // 2, CR // 2)], hfr.at[e, k])
            remote(whole, whole, sh.at[e], hpf.at[e, k], me, mate).start()

        def compute_h(k):
            senders = pl.ds(chunk_of(k, e) * CH, CH)
            acc = jnp.zeros((CR, 256), F32)
            for p in range(NTP):
                x = tok[p, senders, e].reshape(CR, 256)
                acc = acc + jnp.dot(x, wgu[e, p * 256 : (p + 1) * 256, :], preferred_element_type=F32)
            gate, up = acc[:, 0:128], acc[:, 128:256]
            hid[t, e, hrows(k), :] = (gate / (1.0 + jnp.exp(-gate)) * up).astype(BF16)

        def hidden(first, last):
            def step(k):
                pl.when(k < NCH)(lambda: compute_h(k))
                pl.when(k >= 1)(lambda: send_h(k - 1))

            loop(last, step, first)

        def forwarding():
            def step(k):
                pl.when(k < NCH)(lambda: forward_h(k))
                pl.when(k >= 1)(lambda: pass_h(k - 1))

            loop(NCH + 1, step)

        def send_r(k):
            plane = chunk_of(k, e) * 2
            for n in range(CH):
                s = (plane + n // NY) * NY + (my + n) % NY

                def go(s=s):
                    remote(eo.at[e, s], ret[e].at[me], sr.at[e], rr.at[e], s, t).start()

                if n % NY == 0:
                    pl.when(s != me)(go)
                else:
                    go()

        def down_step(k):
            @pl.when(k < NCH)
            def _():
                rows = hrows(k)
                got(hid.at[mate, e, rows], hpo.at[e, k])
                got(hid.at[left + 1 - 2 * mc, e, rows], hpl.at[e, k])
                got(hid.at[right + 1 - 2 * mc, e, rows], hpr.at[e, k])
                got(hid.at[far + 1 - 2 * mc, e, rows], hpf.at[e, k])
                acc = jnp.zeros((CR, 256), F32)
                for q in range(NX):
                    h = jnp.concatenate([hid[2 * q, e, rows, :], hid[2 * q + 1, e, rows, :]], axis=1)
                    acc = acc + jnp.dot(h, wd[e, q * 256 : (q + 1) * 256, :], preferred_element_type=F32)
                eo[e, pl.ds(chunk_of(k, e) * CH, CH)] = acc.astype(BF16).reshape(CH, CAP, 256)

            @pl.when(k >= 1)
            def _():
                send_r(k - 1)

        def returns():
            got(wsend_d.at[e, pl.ds(0, NFS - 1)], rwd.at[e])
            loop(NCH + 1, down_step)
            ret[e][me] = eo[e, me]

        return hidden, forwarding, returns

    hidden_even, forwarding_even, returns_even = phases(0)
    hidden_odd, forwarding_odd, returns_odd = phases(1)
    loop(NZ + 1, gather, NZ)
    loop(3, gathered)
    got(wsend_gu.at[0, pl.ds(0, NFS - 1)], rwgu.at[0])
    hidden_even(0, 1)
    loop(NZ + 2, gather, NZ + 1)
    loop(6, gathered, 3)
    hidden_even(1, 2)
    loop(7, gathered, 6)
    hidden_even(2, 3)
    loop(NZ, gathered, 7)
    hidden_even(3, NCH + 1)
    forwarding_even()
    got(wsend_gu.at[1, pl.ds(0, NFS - 1)], rwgu.at[1])
    hidden_odd(0, NCH + 1)
    returns_even()
    forwarding_odd()
    returns_odd()

    r0, r1 = rt_ref[0:1, :], rt_ref[1:2, :]
    rank0, rank1 = slots[0:1, :] - r0 * CAP, slots[1:2, :] - r1 * CAP
    loads[8].wait()
    a0, a1 = at_ref[0:1, :], at_ref[1:2, :]
    total = a0 + a1

    def keys(r, rank, e):
        key = jnp.right_shift(r, 1) * CAP + rank
        return jnp.where(jnp.bitwise_and(r, 1) == e, key, -1).astype(F32)

    packed = jnp.concatenate(
        [keys(r0, rank0, 0), keys(r1, rank1, 0), keys(r0, rank0, 1), keys(r1, rank1, 1), a0 / total, a1 / total,
         jnp.zeros((122, 768), F32)],
        axis=0,
    )
    macc[...] = jnp.concatenate([packed.T, jnp.zeros((768, 128), F32)], axis=1)

    def weigh(b):
        rows = pl.ds(pl.multiple_of(b * 64, 64), 64)
        columns = macc[rows, 0:128]
        index = lax.broadcasted_iota(jnp.int32, (64, NFS * CAP), 1).astype(F32)
        for e in range(2):
            first = jnp.where(index == columns[:, 2 * e : 2 * e + 1], columns[:, 4:5], 0.0)
            second = jnp.where(index == columns[:, 2 * e + 1 : 2 * e + 2], columns[:, 5:6], 0.0)
            wcomb[e][rows, :] = (first + second).astype(BF16)

    loop(12, weigh)

    got(ret0.at[pl.ds(0, NFS - 1)], rr.at[0])

    def mix_first(b):
        rows = pl.ds(pl.multiple_of(b * 256, 256), 256)
        macc[rows, :] = jnp.dot(wcomb0[rows, :], ret0[...].reshape(NFS * CAP, 256), preferred_element_type=F32)

    loop(3, mix_first)
    got(ret1.at[pl.ds(0, NFS - 1)], rr.at[1])

    for e in range(2):
        sent(wsend_gu.at[e, pl.ds(0, NFS - 1)], swgu.at[e])
        sent(wsend_d.at[e, pl.ds(0, NFS - 1)], swd.at[e])
        sent(hid.at[pl.ds(0, 7), e], sh.at[e])
        sent(eo.at[e, pl.ds(0, NFS - 1)], sr.at[e])
    sent(outbox.at[pl.ds(0, 54)], st)
    sent(blk, sa.at[0])
    sent(near, sa.at[1])
    sent(tok.at[pl.ds(0, 7)], sx)


def finish(wgu, wd, macc, wcomb1, ret1, mixed_out, gate_out, up_out, down_out, mixed, sem):
    copies = [
        pltpu.make_async_copy(wgu.at[:, :, pl.ds(0, 128)], gate_out, sem.at[0]),
        pltpu.make_async_copy(wgu.at[:, :, pl.ds(128, 128)], up_out, sem.at[1]),
        pltpu.make_async_copy(wd, down_out, sem.at[2]),
    ]
    for c in copies:
        c.start()
    for b in range(3):
        rows = pl.ds(b * 256, 256)
        odd = jnp.dot(wcomb1[rows, :], ret1[...].reshape(NFS * CAP, 256), preferred_element_type=F32)
        mixed[rows, :] = (macc[rows, :] + odd).astype(BF16)
    last = pltpu.make_async_copy(mixed, mixed_out, sem.at[3])
    last.start()
    for c in copies + [last]:
        c.wait()


def per_device(prompt, routes, affinity, norm_gain, gate_master, up_master, down_master):
    vmem = pl.BlockSpec(memory_space=pltpu.VMEM)
    hbm = pl.BlockSpec(memory_space=pl.ANY)
    dma = pltpu.SemaphoreType.DMA
    scratch = [
        pltpu.VMEM((2, 768), jnp.int32),
        pltpu.VMEM((2, 768), F32),
        pltpu.VMEM((1, 64), F32),
        pltpu.VMEM((768, 2048), BF16),
        pltpu.VMEM((2, 32, 64, 128), F32),
        pltpu.VMEM((2, 32, 64, 128), F32),
        pltpu.VMEM((2, 32, 32, 256), F32),
        pltpu.VMEM((2, 32, 64, 256), BF16),
        pltpu.VMEM((2, 32, 32, 256), BF16),
        pltpu.VMEM((768, 256), BF16),
        pltpu.VMEM((4, 768, 256), BF16),
        pltpu.VMEM((4, 2, 768), jnp.int32),
        pltpu.VMEM((9 * 8, CAP, 256), BF16),
        pltpu.VMEM((NTP, NFS, 2, CAP, 256), BF16),
        pltpu.VMEM((NTP, 2, NFS * CAP, 128), BF16),
        pltpu.VMEM((2, NFS, CAP, 256), BF16),
        pltpu.VMEM((NFS, CAP, 256), BF16),
        pltpu.VMEM((768, NFS * CAP), BF16),
        pltpu.VMEM((2, 768), jnp.int32),
        dma((10,)),
        dma((2,)), dma((4,)), dma((4,)),
        dma((2,)), dma((2,)), dma((2,)), dma((2,)),
        dma, dma,
        *[dma((NZ,)) for _ in range(9)],
        dma((2,)),
        *[dma((2, 4)) for _ in range(8)],
        dma((2,)), dma((2,)),
    ]
    landed = pl.pallas_call(
        kernel,
        out_shape=(
            pltpu.VMEM((2, 2048, 256), BF16),
            pltpu.VMEM((2, 1024, 256), BF16),
            pltpu.VMEM((768, 256), F32),
            pltpu.VMEM((768, NFS * CAP), BF16),
            pltpu.VMEM((NFS, CAP, 256), BF16),
        ),
        in_specs=[hbm] * 7,
        out_specs=(vmem,) * 5,
        scratch_shapes=scratch,
        compiler_params=pltpu.CompilerParams(
            collective_id=0, has_side_effects=True, vmem_limit_bytes=50 * 1024 * 1024
        ),
        name="hand_off",
    )(
        routes.T,
        affinity.T,
        norm_gain.reshape(1, 64),
        prompt,
        gate_master.reshape(32, 2, 64, 128),
        up_master.reshape(32, 2, 64, 128),
        down_master.reshape(32, 2, 32, 256),
    )
    return pl.pallas_call(
        finish,
        out_shape=(
            jax.ShapeDtypeStruct((768, 256), BF16),
            jax.ShapeDtypeStruct((2, 2048, 128), BF16),
            jax.ShapeDtypeStruct((2, 2048, 128), BF16),
            jax.ShapeDtypeStruct((2, 1024, 256), BF16),
        ),
        in_specs=[vmem] * 5,
        out_specs=(hbm,) * 4,
        scratch_shapes=[pltpu.VMEM((768, 256), BF16), dma((4,))],
        compiler_params=pltpu.CompilerParams(vmem_limit_bytes=8 * 1024 * 1024),
        name="finish",
    )(*landed)


def solution(mesh):
    in_specs = (
        P("fs", None),
        P("fs", None),
        P("fs", None),
        P("fs"),
        P(None, "fs", "tp"),
        P(None, "fs", "tp"),
        P(None, "fs", "tp"),
    )
    out_specs = (P("fs", "tp"), P("fs", None, "tp"), P("fs", None, "tp"), P("fs", None, "tp"))
    return jax.shard_map(
        per_device, mesh=mesh, in_specs=in_specs, out_specs=out_specs, check_vma=False
    )
```
